32 devices in a mesh: sp: 16 (over z, y, core), tp: 2 (over x).
Axes of the slice: x: 2, y: 2, z: 4, core: 2. Of those that a mesh axis runs over, the one named last changes fastest.
Arguments:
- queries: bfloat16 [3072, 1024], P('sp', 'tp'), may hold values from -6 to 6
- keys: bfloat16 [3072, 512], P('sp', 'tp'), may hold values from -6 to 6
- values: bfloat16 [3072, 512], P('sp', 'tp'), may hold values from -6 to 6
- q_gain: float32 [64], replicated, may hold values from 0.1 to 6.5
- k_gain: float32 [64], replicated, may hold values from 0.1 to 6.5
- w_out: bfloat16 [1024, 2048], P('tp'), may hold values from -12 to 12
- residual: bfloat16 [3072, 2048], P(('sp', 'tp')), may hold values from -6 to 6
- norm_gain: float32 [2048], replicated, may hold values from 0.1 to 1.9
- w_gate: bfloat16 [2048, 5632], P('sp', 'tp'), may hold values from -0.125 to 0.125
- w_up: bfloat16 [2048, 5632], P('sp', 'tp'), may hold values from -0.125 to 0.125
- w_down: bfloat16 [5632, 2048], P('tp', 'sp'), may hold values from -0.25 to 0.25
Outputs:
- layer_out: bfloat16 [3072, 2048], P(('sp', 'tp'))
The draws below stay inside these ranges and needn't reach their ends.
All inputs are finite; a program needn't handle non-finite values.
Results may differ from the reference program's by a relative error of at most 0.018.
The reference program's roundings to bfloat16 on the way count: a program that leaves them out, or rounds other values in their place, can miss the bound.
Values may be sent and summed in bfloat16 or wider, within the bound.
A program may use at most 128 MiB of HBM per device.

```python
import math
import jax
import jax.numpy as jnp
from jax import lax

D = 2048
FF = 5632
HEADS = 16
KV_HEADS = 8
HEAD = 64
GRID_W = 128
TOKENS = 3072
ATTN = 1024
KV_WIDTH = 512


def draw_queries(key, part):
    base = jnp.clip(jax.random.normal(jax.random.fold_in(key, 11), (TOKENS, HEADS * HEAD), jnp.float32), -6.0, 6.0)
    return base.astype(jnp.bfloat16)


def draw_keys(key, part):
    base = jnp.clip(jax.random.normal(jax.random.fold_in(key, 23), (TOKENS, KV_HEADS * HEAD), jnp.float32), -6.0, 6.0)
    return base.astype(jnp.bfloat16)


def draw_q_gain(key, part):
    return jax.random.uniform(jax.random.fold_in(key, 53), (HEAD,), jnp.float32, 0.1, 1.9)


def draw_k_gain(key, part):
    return jax.random.uniform(jax.random.fold_in(key, 63), (HEAD,), jnp.float32, 0.1, 1.9)


def draw_w_out(key, part):
    base = jax.random.normal(jax.random.fold_in(key, 71), (HEADS * HEAD, D), jnp.float32)
    return jnp.clip(base * 2.0, -12.0, 12.0).astype(jnp.bfloat16)


def steps_of(stream_key, shape, cuts, least, largest):
    def one(axis_at, blocks):
        steps = jax.random.uniform(jax.random.fold_in(jax.random.fold_in(stream_key, 6), axis_at), (blocks,), jnp.float32, least / len(cuts), largest / len(cuts))
        return jnp.repeat(jnp.exp(steps), shape[axis_at] // blocks).reshape((-1,) + (1,) * (len(shape) - axis_at - 1))

    factor_of = one(*cuts[0])
    for cut in cuts[1:]:
        factor_of = factor_of * one(*cut)
    return factor_of


def centred(rng, shape, spread, limit, shards=(), held_as=jnp.bfloat16):
    factor_of = steps_of(rng, shape, shards, -0.22, 0.18) if shards else 1.0
    array = jax.random.normal(rng, shape, jnp.float32) * spread * factor_of
    return jnp.minimum(jnp.maximum(array, -limit), limit).astype(held_as)


def setup_inputs(seed: int = 0) -> dict:
    splits = jax.random.split(jax.random.key(seed), 12)
    return {
        "queries": draw_queries(jax.random.fold_in(splits[11], 71), 0),
        "keys": draw_keys(jax.random.fold_in(splits[11], 71), 0),
        "values": centred(splits[2], (TOKENS, KV_WIDTH), 1.0, 6.0, ((0, 16), (1, 2))),
        "q_gain": draw_q_gain(jax.random.fold_in(splits[11], 71), 0),
        "k_gain": draw_k_gain(jax.random.fold_in(splits[11], 71), 0),
        "w_out": draw_w_out(jax.random.fold_in(splits[11], 71), 0),
        "residual": centred(splits[6], (TOKENS, D), 1.0, 6.0, ((0, 32),)),
        "norm_gain": jnp.clip(1.0 + 0.18 * jax.random.normal(splits[7], (D,), jnp.float32), 0.1, 1.9),
        "w_gate": centred(splits[8], (D, FF), D ** -0.5, 0.125, ((0, 16), (1, 2))),
        "w_up": centred(splits[9], (D, FF), D ** -0.5, 0.125, ((0, 16), (1, 2))),
        "w_down": centred(splits[10], (FF, D), (FF // 9) ** -0.5, 0.25, ((0, 2), (1, 16))),
    }


EPS = 1e-06
THETA = 10000.0

def turn_half(part, angle):
    quarter = part.shape[-1] // 2
    cos_table = jnp.cos(angle)[:, None, :]
    sin_table = jnp.sin(angle)[:, None, :]
    first_part = part[..., :quarter]
    second_part = part[..., quarter:]
    return jnp.concatenate([first_part * cos_table - second_part * sin_table, first_part * sin_table + second_part * cos_table], axis=-1)

def head_norm_rope(flat, gain, offset, head_count):
    tok_rows = flat.shape[0]
    head_size = flat.shape[1] // head_count
    heads = flat.astype(jnp.float32).reshape(tok_rows, head_count, head_size)
    heads = heads * lax.rsqrt(lax.optimization_barrier(jnp.mean(heads * heads, axis=-1, keepdims=True)) + EPS) * gain.astype(jnp.float32)
    positions = offset + jnp.arange(tok_rows, dtype=jnp.int32)
    row_pos = (positions // GRID_W).astype(jnp.float32)
    col_pos = (positions % GRID_W).astype(jnp.float32)
    half_size = head_size // 2
    inv_freq = THETA ** (-jnp.arange(0, half_size, 2, dtype=jnp.float32) / half_size)
    turned = jnp.concatenate([turn_half(heads[..., :half_size], row_pos[:, None] * inv_freq[None, :]), turn_half(heads[..., half_size:], col_pos[:, None] * inv_freq[None, :])], axis=-1)
    return turned.reshape(tok_rows, head_count * head_size).astype(jnp.bfloat16)

def reference(queries, keys, values, q_gain, k_gain, w_out, residual, norm_gain, w_gate, w_up, w_down):
    q_group = HEADS // KV_HEADS
    q_rot = head_norm_rope(queries, q_gain, 0, HEADS)
    k_rot = head_norm_rope(keys, k_gain, 0, KV_HEADS)
    key_heads = k_rot.reshape(TOKENS, KV_HEADS, HEAD).astype(jnp.float32)
    value_heads = values.reshape(TOKENS, KV_HEADS, HEAD).astype(jnp.float32)
    block_len = math.gcd(TOKENS, 256)
    query_blocks = q_rot.reshape(TOKENS // block_len, block_len, KV_HEADS, q_group, HEAD)
    score_scale = HEAD ** (-0.5)

    def attend_block(query_block):
        scores = jnp.einsum('qhgd,khd->hgqk', query_block.astype(jnp.float32), key_heads) * score_scale
        top = lax.optimization_barrier(jnp.max(scores, axis=-1, keepdims=True))
        weights = jnp.exp(scores - top)
        totals = lax.optimization_barrier(jnp.sum(weights, axis=-1))
        rounded = weights.astype(jnp.bfloat16).astype(jnp.float32)
        mixed = jnp.einsum('hgqk,khd->qhgd', rounded, value_heads)
        mixed = mixed / jnp.transpose(totals, (2, 0, 1))[..., None]
        return mixed.astype(jnp.bfloat16).reshape(block_len, ATTN)
    attn = lax.map(attend_block, query_blocks).reshape(TOKENS, ATTN)
    proj = jnp.dot(attn, w_out, preferred_element_type=jnp.float32)
    mid = residual.astype(jnp.float32) + proj
    normed = (mid * lax.rsqrt(lax.optimization_barrier(jnp.mean(mid * mid, axis=-1, keepdims=True)) + EPS) * norm_gain.astype(jnp.float32)).astype(jnp.bfloat16)
    gate = jnp.dot(normed, w_gate, preferred_element_type=jnp.float32)
    up_part = jnp.dot(normed, w_up, preferred_element_type=jnp.float32)
    hidden = (jax.nn.silu(gate) * up_part).astype(jnp.bfloat16)
    down = jnp.dot(hidden, w_down, preferred_element_type=jnp.float32)
    return (mid + 0.5 * down).astype(jnp.bfloat16)
```

```python
import functools
import math

import jax
import jax.numpy as jnp
from jax import lax
from jax.experimental import pallas as pl
from jax.experimental.pallas import tpu as pltpu
from jax.sharding import PartitionSpec as P

GRID_W = 128


EPS = 1e-06
THETA = 10000.0


def turn_half(part, angle):
    quarter = part.shape[-1] // 2
    cos_table = jnp.cos(angle)[:, None, :]
    sin_table = jnp.sin(angle)[:, None, :]
    first_part = part[..., :quarter]
    second_part = part[..., quarter:]
    return jnp.concatenate(
        [
            first_part * cos_table - second_part * sin_table,
            first_part * sin_table + second_part * cos_table,
        ],
        axis=-1,
    )


def head_norm_rope(flat, gain, offset, head_count):
    tok_rows = flat.shape[0]
    head_size = flat.shape[1] // head_count
    heads = flat.astype(jnp.float32).reshape(tok_rows, head_count, head_size)
    heads = heads * lax.rsqrt(jnp.mean(heads * heads, axis=-1, keepdims=True) + EPS) * gain
    positions = offset + jnp.arange(tok_rows, dtype=jnp.int32)
    row_pos = (positions // GRID_W).astype(jnp.float32)
    col_pos = (positions % GRID_W).astype(jnp.float32)
    half_size = head_size // 2
    inv_freq = THETA ** (-jnp.arange(0, half_size, 2, dtype=jnp.float32) / half_size)
    turned = jnp.concatenate(
        [
            turn_half(heads[..., :half_size], row_pos[:, None] * inv_freq[None, :]),
            turn_half(heads[..., half_size:], col_pos[:, None] * inv_freq[None, :]),
        ],
        axis=-1,
    )
    return turned.reshape(tok_rows, head_count * head_size).astype(jnp.bfloat16)


def body(queries, keys, values, q_gain, k_gain, w_out, residual, norm_gain, w_gate, w_up, w_down):
    tok_rows = queries.shape[0]
    head_size = q_gain.shape[0]
    q_heads = queries.shape[1] // head_size
    kv_heads = keys.shape[1] // head_size
    q_group = q_heads // kv_heads
    offset = lax.axis_index("sp") * tok_rows
    q_rot = head_norm_rope(queries, q_gain, offset, q_heads)
    k_rot = head_norm_rope(keys, k_gain, offset, kv_heads)
    query_groups = q_rot.reshape(tok_rows, kv_heads, q_group, head_size)
    score_scale = head_size ** (-0.5)
    start_state = (
        jnp.full((kv_heads, q_group, tok_rows), -1e30, jnp.float32),
        jnp.zeros((kv_heads, q_group, tok_rows), jnp.float32),
        jnp.zeros((kv_heads, q_group, tok_rows, head_size), jnp.float32),
    )
    running = start_state
    key_piece = lax.all_gather(k_rot, "sp", axis=0, tiled=True)
    value_piece = lax.all_gather(values, "sp", axis=0, tiled=True)
    piece_len = key_piece.shape[0]
    block_len = math.gcd(piece_len, 512)
    blocks = piece_len // block_len
    key_blocks = key_piece.reshape(blocks, block_len, kv_heads, head_size)
    value_blocks = value_piece.reshape(blocks, block_len, kv_heads, head_size)

    def update(state, block_pair):
        prior_max, totals, accum = state
        key_block, value_block = block_pair
        scores = (
            jnp.einsum(
                "qhgd,khd->hgqk", query_groups, key_block, preferred_element_type=jnp.float32
            )
            * score_scale
        )
        new_max = jnp.maximum(prior_max, jnp.max(scores, axis=-1))
        weights = jnp.exp(scores - new_max[..., None])
        factor = jnp.exp(prior_max - new_max)
        totals = totals * factor + jnp.sum(weights, axis=-1)
        accum = accum * factor[..., None] + jnp.einsum(
            "hgqk,khd->hgqd",
            weights.astype(jnp.bfloat16),
            value_block,
            preferred_element_type=jnp.float32,
        )
        return ((new_max, totals, accum), None)

    running, unused = lax.scan(update, running, (key_blocks, value_blocks))
    final_max, totals, accum = running
    mixed = accum / totals[..., None]
    attn = (
        jnp.transpose(mixed, (2, 0, 1, 3))
        .reshape(tok_rows, q_heads * head_size)
        .astype(jnp.bfloat16)
    )
    own_rows = lax.all_to_all(attn, "tp", split_axis=0, concat_axis=1, tiled=True)
    columns = own_rows
    proj = jnp.dot(
        columns, lax.all_gather(w_out, "tp", axis=0, tiled=True), preferred_element_type=jnp.float32
    )
    mid = residual.astype(jnp.float32) + proj
    normed = (
        mid * lax.rsqrt(jnp.mean(mid * mid, axis=-1, keepdims=True) + EPS) * norm_gain
    ).astype(jnp.bfloat16)
    gathered = lax.all_gather(normed, "tp", axis=0, tiled=True)
    columns = gathered
    gate = jnp.dot(
        columns,
        lax.all_gather(w_gate, "sp", axis=0, tiled=True),
        preferred_element_type=jnp.float32,
    )
    up_part = jnp.dot(
        columns, lax.all_gather(w_up, "sp", axis=0, tiled=True), preferred_element_type=jnp.float32
    )
    hidden = (jax.nn.silu(gate) * up_part).astype(jnp.bfloat16)
    terms = jnp.dot(
        hidden, lax.all_gather(w_down, "sp", axis=1, tiled=True), preferred_element_type=jnp.float32
    )
    down = lax.psum_scatter(
        terms.astype(jnp.bfloat16), "tp", scatter_dimension=0, tiled=True
    ).astype(jnp.float32)
    return (mid + 0.5 * down).astype(jnp.bfloat16)


MESH = pl.DeviceIdType.MESH
BLOCK = 128


def line_of_chips(mesh):
    count = mesh.shape["sp"]
    try:
        places = [(tuple(d.coords), d.core_on_chip) for d in mesh.devices[:, 0].flat]
    except AttributeError:
        return None
    if count % 4 or count < 12 or mesh.shape["tp"] != 2:
        return None
    first = places[0][0]
    for at, (coords, core) in enumerate(places):
        chip = at // 2
        want = (first[0], first[1] + chip % 2, first[2] + chip // 2)
        if coords != want or core != at % 2:
            return None
    return count // 4


def message_count(n):
    events = 2 * (n - 1)
    return 9 * (events + 1) + 2 * events + 12 * n + 3 + 4 * events + 6 * n + n + 2


def slab_width(units, n):
    blocks = units // BLOCK
    return -(-blocks // n) * BLOCK


def turned_heads(head_size, x_ref, g_ref, cos_ref, sin_ref):
    x = x_ref[...].astype(jnp.float32)
    width = x.shape[1]
    lane = lax.broadcasted_iota(jnp.int32, (width, width), 0) // head_size
    other = lax.broadcasted_iota(jnp.int32, (width, width), 1) // head_size
    same = (lane == other).astype(jnp.float32)
    mean = jnp.dot(
        x * x, same, preferred_element_type=jnp.float32, precision=lax.Precision.HIGHEST
    ) * (1.0 / head_size)
    h = x * lax.rsqrt(mean + EPS) * jnp.concatenate([g_ref[...]] * (width // head_size), axis=1)
    quarter = head_size // 4
    repeats = width // cos_ref.shape[1]
    cos_table = jnp.concatenate([cos_ref[...]] * repeats, axis=1)
    sin_table = jnp.concatenate([sin_ref[...]] * repeats, axis=1)
    at = lax.broadcasted_iota(jnp.int32, x.shape, 1)
    is_first = (at // quarter) % 2 == 0
    ahead = pltpu.roll(h, width - quarter, 1)
    behind = pltpu.roll(h, quarter, 1)
    turned = h * cos_table + jnp.where(is_first, -ahead, behind) * sin_table
    return turned.astype(jnp.bfloat16)


def when(condition, action):
    if condition is None:
        action()
    else:
        pl.when(condition)(action)


def both(one, other):
    if one is None:
        return other
    if other is None:
        return one
    return jnp.logical_and(one, other)


def layer_kernel(
    n, head_size,
    raw_q, raw_k, raw_v, qg_ref, kg_ref, cos_ref, sin_ref, res_ref, gain_ref, wo_in, wg_in, wu_in, wd_in,
    out_ref,
    q_ref, kv_all, wg_all, wu_all, wd_all, wo_own, wo_other, attn, context, context_in, mid, normed, hidden,
    part, leaving, line_in, pair_in, own_sem, send_sem, recv_sem,
):
    sp = lax.axis_index("sp")
    tp = lax.axis_index("tp")
    core = lax.rem(sp, 2)
    y = lax.rem(lax.div(sp, 2), 2)
    z = lax.div(sp, 4)

    def device(zz, yy, cc):
        return (zz * 2 + yy) * 2 + cc

    def wrapped(zz):
        return lax.rem(zz + n, n)

    sibling = (device(z, y, 1 - core), tp)
    across = (device(z, 1 - y, core), tp)
    partner = (sp, 1 - tp)

    def level(zz):
        return (device(zz, y, core), tp)

    barrier = pltpu.get_barrier_semaphore()
    greeted = [sibling, across, partner] + [level(wrapped(z + d)) for d in range(1, n)]
    for target in greeted:
        pl.semaphore_signal(barrier, inc=1, device_id=target, device_id_type=MESH)
    pl.semaphore_wait(barrier, len(greeted))

    slots = {}
    sent = []

    def message(key, src, dst, target):
        slot = slots.setdefault(key, len(slots))
        return pltpu.make_async_remote_copy(
            src_ref=src, dst_ref=dst, send_sem=send_sem.at[slot], recv_sem=recv_sem.at[slot],
            device_id=target, device_id_type=MESH,
        )

    def send(key, condition, src, dst, target):
        def make():
            return message(key, src(), dst(), target)

        when(condition, lambda: make().start())
        sent.append((condition, make))

    def land(key, condition, piece):
        when(condition, lambda: message(key, piece(), piece(), partner).wait_recv())

    arrivals = [[(s, w) for w in range(2)] for s in range(n - 1)]
    events = [None] + [e for step in arrivals for e in step]
    room = (z <= n - 2, z >= 1)
    ahead = (level(z + 1), level(z - 1))

    def home(e):
        if e is None:
            return z
        return z - 1 - e[0] if e[1] == 0 else z + 1 + e[0]

    def real(e):
        if e is None:
            return None
        return z >= e[0] + 1 if e[1] == 0 else z <= n - 2 - e[0]

    def pass_on(name, e, src, dst):
        for w in range(2) if e is None else (e[1],):
            step = 0 if e is None else e[0] + 1
            if step <= n - 2:
                send((name, step, w), both(real(e), room[w]), src, dst, ahead[w])

    tok = raw_q.shape[0]
    kv_width = raw_k.shape[1]

    def kv_piece(j, zz, yy, cc):
        start = pl.multiple_of(device(zz, yy, cc) * tok, tok)
        return kv_all.at[pl.ds(start, tok), j * kv_width:(j + 1) * kv_width]

    def kv_serve(j, e):
        def dst():
            return kv_piece(j, home(e), y, core)

        if e is not None:
            land((("kv", j), e[0], e[1]), real(e), dst)
        src = (lambda: raw_v) if e is None and j == 1 else dst
        pass_on(("kv", j), e, src, dst)
        send(("kv y", j, e), real(e), src, dst, across)
        send(("kv core", j, e, 0), real(e), src, dst, sibling)

    def kv_cross(j, e):
        def piece():
            return kv_piece(j, home(e), 1 - y, core)

        land(("kv y", j, e), real(e), piece)
        send(("kv core", j, e, 1), real(e), piece, piece, sibling)

    def kv_finish(j, e):
        land(("kv core", j, e, 0), real(e), lambda: kv_piece(j, home(e), y, 1 - core))
        land(("kv core", j, e, 1), real(e), lambda: kv_piece(j, home(e), 1 - y, 1 - core))

    GATE, UP, DOWN = range(3)
    weights_in = (wg_in, wu_in, wd_in)
    rows, units = wg_in.shape
    lanes_down = wd_in.shape[1]
    blocks = units // BLOCK
    slab = wg_all.shape[1]

    def first_block(zz):
        return lax.div(zz * blocks, n)

    def weight_in(k, zz):
        span = pl.ds(pl.multiple_of(first_block(zz) * BLOCK, BLOCK), slab)
        return wd_in.at[span, :] if k == DOWN else weights_in[k].at[:, span]

    def weight(k, zz, yy, cc):
        o = device(zz, yy, cc)
        if k == DOWN:
            return wd_all.at[:, pl.ds(pl.multiple_of(o * lanes_down, lanes_down), lanes_down)]
        return (wg_all, wu_all)[k].at[pl.ds(pl.multiple_of(o * rows, rows), rows), :]

    def weight_line(k, d):
        zt = wrapped(z + d)
        send(
            ("w z", k, d), None,
            lambda: weight_in(k, zt), lambda: weight(k, z, y, core), level(zt),
        )

    def weight_serve(k, d):
        zs = wrapped(z - d)

        def dst():
            return weight(k, zs, y, core)

        src = dst
        if d == 0:
            src = lambda: weight_in(k, z)
        else:
            land(("w z", k, d), None, dst)
        send(("w y", k, d), None, src, dst, across)
        send(("w core", k, d, 0), None, src, dst, sibling)

    def weight_cross(k, d):
        def piece():
            return weight(k, wrapped(z - d), 1 - y, core)

        land(("w y", k, d), None, piece)
        send(("w core", k, d, 1), None, piece, piece, sibling)

    own = [
        pltpu.make_async_copy(weight_in(k, z), weight(k, z, y, core), own_sem.at[k]) for k in range(3)
    ] + [pltpu.make_async_copy(wo_in, wo_own, own_sem.at[3])]

    def weight_finish(k):
        own[k].wait()
        for d in range(n):
            zs = wrapped(z - d)
            land(("w core", k, d, 0), None, lambda: weight(k, zs, y, 1 - core))
            land(("w core", k, d, 1), None, lambda: weight(k, zs, 1 - y, 1 - core))

    wo_half = wo_in.shape[0] // 2

    def wo_part(ref, cc):
        return ref.at[pl.ds(pl.multiple_of(cc * wo_half, wo_half), wo_half), :]

    pairs, q_rows, lanes = q_ref.shape
    block = math.gcd(q_rows, 256)
    per_pair = q_rows // block

    def attend(at):
        pair, which = at // per_pair, at % per_pair
        span = slice(which * block, (which + 1) * block)
        q = q_ref[pair, span, :]
        k = kv_all[:, pair * lanes:(pair + 1) * lanes]
        v = kv_all[:, (pairs + pair) * lanes:(pairs + pair + 1) * lanes]
        scores = lax.dot_general(
            q, k, (((1,), (1,)), ((), ())), preferred_element_type=jnp.float32
        )
        weights = jnp.exp(scores - jnp.max(scores, axis=-1, keepdims=True))
        total = jnp.sum(weights, axis=-1, keepdims=True)
        mixed = jnp.dot(weights.astype(jnp.bfloat16), v, preferred_element_type=jnp.float32)
        attn[pair, span, :] = (mixed / total).astype(jnp.bfloat16)

    def assemble():
        group = q_rows // (2 * tok)
        pieces = []
        for pair in range(pairs):
            for side in range(2):
                for g in range(0, group, 2):
                    lower = attn[pair, pl.ds((side * group + g) * tok, tok), :].astype(jnp.float32)
                    upper = attn[pair, pl.ds((side * group + g + 1) * tok, tok), :].astype(jnp.float32)
                    if side == 1:
                        lower = pltpu.roll(lower, head_size, 1)
                    else:
                        upper = pltpu.roll(upper, head_size, 1)
                    lane = lax.broadcasted_iota(jnp.int32, lower.shape, 1)
                    pieces.append(jnp.where(lane < head_size, lower, upper).astype(jnp.bfloat16))
        context[...] = jnp.concatenate(pieces, axis=1)

    own_count, width = res_ref.shape
    rows_of = own_count // 2
    mine = pl.ds(pl.multiple_of(tp * own_count, own_count), own_count)
    theirs = pl.ds(pl.multiple_of((1 - tp) * own_count, own_count), own_count)

    def span_of(zz, f):
        xx, part_of = ((tp, 0), (tp, 1), (1 - tp, 1), (1 - tp, 0))[f]
        start = ((zz * 2 + xx) * 2 + part_of) * rows_of
        return pl.ds(pl.multiple_of(start, rows_of), rows_of)

    def normalize():
        held, other = context[mine, :], context_in[...]
        wide = math.gcd(width, 512)
        for at in range(0, width, wide):
            cols = slice(at, at + wide)
            mid[:, cols] = res_ref[:, cols].astype(jnp.float32) + (
                jnp.dot(held, wo_own[:, cols], preferred_element_type=jnp.float32)
                + jnp.dot(other, wo_other[:, cols], preferred_element_type=jnp.float32)
            )
        value = mid[...]
        scale = lax.rsqrt(jnp.mean(value * value, axis=-1, keepdims=True) + EPS)
        result = (value * scale * gain_ref[...]).astype(jnp.bfloat16)
        normed[span_of(z, 0), :] = result[:rows_of]
        normed[span_of(z, 1), :] = result[rows_of:]

    def rows_serve(f, e):
        def piece():
            return normed.at[span_of(home(e), f), :]

        if e is not None:
            land((("rows", f), e[0], e[1]), real(e), piece)
        elif f == 2:
            land(("rows x", "second"), None, piece)
        pass_on(("rows", f), e, piece, piece)
        if f == 0:
            send(("rows x", e), real(e), piece, piece, partner)
        if f == 1 and e is None:
            send(("rows x", "second"), None, piece, piece, partner)

    def rows_cross(e):
        land(("rows x", e), real(e), lambda: normed.at[span_of(home(e), 3), :])

    def nearest(p):
        result = 0
        for zz in range(n):
            order = sorted(range(n), key=lambda other: (abs(other - zz), other))
            result = jnp.where(z == zz, order[p], result)
        return result

    piece_rows = 2 * own_count
    tile = math.gcd(slab, 256)
    valid = (first_block(z + 1) - first_block(z)) * BLOCK

    def feed(p):
        start = pl.multiple_of(nearest(p) * piece_rows, piece_rows)

        @pl.loop(0, slab // tile)
        def _(at):
            cols = pl.ds(pl.multiple_of(at * tile, tile), tile)
            x = normed[pl.ds(start, piece_rows), :]
            gate = jnp.dot(x, wg_all[:, cols], preferred_element_type=jnp.float32)
            up = jnp.dot(x, wu_all[:, cols], preferred_element_type=jnp.float32)
            unit = at * tile + lax.broadcasted_iota(jnp.int32, gate.shape, 1)
            product = jnp.where(unit < valid, gate / (1.0 + jnp.exp(-gate)) * up, 0.0)
            hidden[p * piece_rows:(p + 1) * piece_rows, cols] = product.astype(jnp.bfloat16)

    wide_down = math.gcd(width, 512)

    def lower(p):
        zz = nearest(p)
        start = pl.multiple_of(zz * piece_rows, piece_rows)

        @pl.loop(0, width // wide_down)
        def _(at):
            cols = pl.ds(pl.multiple_of(at * wide_down, wide_down), wide_down)
            part[pl.ds(start, piece_rows), cols] = jnp.dot(
                hidden[p * piece_rows:(p + 1) * piece_rows, :], wd_all[:, cols],
                preferred_element_type=jnp.float32,
            )

        leaving[span_of(zz, 3), :] = part[span_of(zz, 3), :].astype(jnp.bfloat16)
        send(
            ("sum x", p), None,
            lambda: leaving.at[span_of(zz, 3), :], lambda: pair_in.at[zz], partner,
        )

    def add(zz, f, ref):
        part[span_of(zz, f), :] = part[span_of(zz, f), :] + ref[...].astype(jnp.float32)

    def sum_send(f, w, d):
        zz = z + d if w == 0 else z - d
        inside = z <= n - 1 - d if w == 0 else z >= d
        if d < n - 1:
            def take():
                message(("sum", f, w, d + 1), line_in.at[f, w, d], line_in.at[f, w, d], partner).wait_recv()
                add(zz, f, line_in.at[f, w, d])

            when(both(inside, room[1 - w]), take)

        def put():
            leaving[span_of(zz, f), :] = part[span_of(zz, f), :].astype(jnp.bfloat16)

        when(inside, put)
        send(
            ("sum", f, w, d), inside,
            lambda: leaving.at[span_of(zz, f), :], lambda: line_in.at[f, w, d - 1], ahead[w],
        )

    def sum_finish(f):
        for w in range(2):
            def take():
                message(("sum", f, w, 1), line_in.at[f, w, 0], line_in.at[f, w, 0], partner).wait_recv()
                add(z, f, line_in.at[f, w, 0])

            when(room[1 - w], take)

    for copy in own:
        copy.start()
    kv_serve(1, None)
    send(
        ("wo", 0), None, lambda: wo_part(wo_in, core), lambda: wo_part(wo_other, core), partner
    )
    weight_line(GATE, 1)
    own_rows = pl.ds(pl.multiple_of(sp * tok, tok), tok)
    kv_all[own_rows, :kv_width] = turned_heads(head_size, raw_k, kg_ref, cos_ref, sin_ref)
    kv_all[own_rows, kv_width:] = raw_v[...]
    kv_serve(0, None)
    turned = turned_heads(head_size, raw_q, qg_ref, cos_ref, sin_ref).astype(jnp.float32)
    turned = turned * head_size ** (-0.5)
    group = q_rows // (2 * tok)
    for at in range(raw_q.shape[1] // lanes):
        together = turned[:, at * lanes:(at + 1) * lanes]
        swapped = pltpu.roll(together, head_size, 1)
        low = lax.broadcasted_iota(jnp.int32, together.shape, 1) < head_size
        key_head, g = 2 * at // group, 2 * at % group
        pair, side = key_head // 2, key_head % 2
        for extra in range(2):
            source = together if extra == side else swapped
            kept_lanes = jnp.where(low if side == 0 else jnp.logical_not(low), source, 0.0)
            first = (side * group + g + extra) * tok
            q_ref[pair, first:first + tok, :] = kept_lanes.astype(jnp.bfloat16)

    lines = [(k, d) for k in range(3) for d in range(1, n)][1:]
    crossing = [None]
    for step in arrivals:
        for j in (1, 0):
            for e in step:
                kv_serve(j, e)
        weight_line(*lines.pop(0))
        for j in (1, 0):
            for e in crossing:
                kv_cross(j, e)
        crossing = step
    for k, d in lines:
        weight_line(k, d)
    weight_serve(GATE, 0)
    for j in (1, 0):
        for e in crossing:
            kv_cross(j, e)
    for j in (1, 0):
        for e in events:
            kv_finish(j, e)

    tasks = []
    served = [(k, d) for k in range(3) for d in range(n)]
    for at in range(1, len(served)):
        tasks.append((weight_serve, served[at]))
        tasks.append((weight_cross, served[at - 1]))
    tasks.append((weight_cross, served[-1]))

    def work(count):
        for _ in range(min(count, len(tasks))):
            task, what = tasks.pop(0)
            task(*what)

    for at in range(pairs * per_pair):
        attend(at)
        work(2)
        if at == 2:
            land(("wo", 0), None, lambda: wo_part(wo_other, core))
            send(
                ("wo", 1), None,
                lambda: wo_part(wo_other, core), lambda: wo_part(wo_other, core), sibling,
            )
    assemble()
    work(1)
    send(("context",), None, lambda: context.at[theirs, :], lambda: context_in, partner)
    work(1)
    land(("wo", 1), None, lambda: wo_part(wo_other, 1 - core))
    own[3].wait()
    land(("context",), None, lambda: context_in)
    normalize()
    work(1)
    for f in (0, 1):
        rows_serve(f, None)
    work(1)
    rows_serve(2, None)
    rows_cross(None)
    work(len(tasks))
    weight_finish(GATE)
    weight_finish(UP)
    feed(0)
    for at, step in enumerate(arrivals):
        for f in range(3):
            for e in step:
                rows_serve(f, e)
        if at == 0:
            weight_finish(DOWN)
            lower(0)
        for e in step:
            rows_cross(e)
        feed(at + 1)
        lower(at + 1)
    for p in range(n):
        zz = nearest(p)
        land(("sum x", p), None, lambda: pair_in.at[zz])
        add(zz, 0, pair_in.at[zz])
    for d in range(n - 1, 0, -1):
        for f in (1, 2, 0):
            for w in range(2):
                sum_send(f, w, d)
    sum_finish(2)
    leaving[span_of(z, 2), :] = part[span_of(z, 2), :].astype(jnp.bfloat16)
    sum_finish(0)
    out_ref[:rows_of, :] = (mid[:rows_of, :] + 0.5 * part[span_of(z, 0), :]).astype(jnp.bfloat16)
    send(("sum x", "second"), None, lambda: leaving.at[span_of(z, 2), :], lambda: pair_in.at[n], partner)
    sum_finish(1)
    land(("sum x", "second"), None, lambda: pair_in.at[n])
    add(z, 1, pair_in.at[n])
    out_ref[rows_of:, :] = (mid[rows_of:, :] + 0.5 * part[span_of(z, 1), :]).astype(jnp.bfloat16)
    for condition, make in sent:
        when(condition, lambda: make().wait_send())
    assert len(slots) <= send_sem.shape[0]


def fast_body(n, queries, keys, values, q_gain, k_gain, w_out, residual, norm_gain, w_gate, w_up, w_down):
    tok_rows = queries.shape[0]
    head_size = q_gain.shape[0]
    q_heads = queries.shape[1] // head_size
    kv_heads = keys.shape[1] // head_size
    q_group = q_heads // kv_heads
    n_sp = 4 * n
    positions = lax.axis_index("sp") * tok_rows + jnp.arange(tok_rows, dtype=jnp.int32)
    half_size = head_size // 2
    inv_freq = THETA ** (-jnp.arange(0, half_size, 2, dtype=jnp.float32) / half_size)
    row_angle = (positions // GRID_W).astype(jnp.float32)[:, None] * inv_freq[None, :]
    col_angle = (positions % GRID_W).astype(jnp.float32)[:, None] * inv_freq[None, :]
    angle = jnp.concatenate([row_angle, row_angle, col_angle, col_angle] * 2, axis=1)
    cos_table, sin_table = jnp.cos(angle), jnp.sin(angle)
    pairs = kv_heads // 2
    padded = (pairs, 2 * q_group * tok_rows, 2 * head_size)
    kv_width = keys.shape[1] + values.shape[1]
    tokens = n_sp * tok_rows
    any_space = pl.BlockSpec(memory_space=pl.ANY)
    vmem = pl.BlockSpec(memory_space=pltpu.VMEM)
    own_count, width = residual.shape
    depth_in, units = w_gate.shape
    lanes_down = w_down.shape[1]
    slab = slab_width(units, n)
    group_rows = 2 * n * own_count
    bf16, f32 = jnp.bfloat16, jnp.float32
    return pl.pallas_call(
        functools.partial(layer_kernel, n, head_size),
        out_shape=jax.ShapeDtypeStruct(residual.shape, bf16),
        in_specs=[vmem] * 9 + [any_space] * 4,
        out_specs=vmem,
        scratch_shapes=[
            pltpu.VMEM(padded, bf16),
            pltpu.VMEM((tokens, kv_width), bf16),
            pltpu.VMEM((n_sp * depth_in, slab), bf16),
            pltpu.VMEM((n_sp * depth_in, slab), bf16),
            pltpu.VMEM((slab, n_sp * lanes_down), bf16),
            pltpu.VMEM(w_out.shape, bf16),
            pltpu.VMEM(w_out.shape, bf16),
            pltpu.VMEM(padded, bf16),
            pltpu.VMEM(queries.shape, bf16),
            pltpu.VMEM((own_count, queries.shape[1]), bf16),
            pltpu.VMEM((own_count, width), f32),
            pltpu.VMEM((group_rows, width), bf16),
            pltpu.VMEM((group_rows, slab), bf16),
            pltpu.VMEM((group_rows, width), f32),
            pltpu.VMEM((group_rows, width), bf16),
            pltpu.VMEM((3, 2, n - 1, own_count // 2, width), bf16),
            pltpu.VMEM((n + 1, own_count // 2, width), bf16),
            pltpu.SemaphoreType.DMA((4,)),
            pltpu.SemaphoreType.DMA((message_count(n),)),
            pltpu.SemaphoreType.DMA((message_count(n),)),
        ],
        compiler_params=pltpu.CompilerParams(
            collective_id=0, has_side_effects=True, vmem_limit_bytes=63 * 1024 * 1024
        ),
        name="layer",
    )(
        queries, keys, values, q_gain[None, :], k_gain[None, :], cos_table, sin_table,
        residual, norm_gain[None, :], w_out, w_gate, w_up, w_down)


def solution(mesh):
    n = line_of_chips(mesh)
    inner = body if n is None else functools.partial(fast_body, n)
    return jax.shard_map(
        inner,
        mesh=mesh,
        in_specs=(
            P("sp", "tp"),
            P("sp", "tp"),
            P("sp", "tp"),
            P(),
            P(),
            P("tp", None),
            P(("sp", "tp"), None),
            P(),
            P("sp", "tp"),
            P("sp", "tp"),
            P("tp", "sp"),
        ),
        out_specs=P(("sp", "tp"), None),
        check_vma=False,
    )
```

```python
import functools
import math

import jax
import jax.numpy as jnp
from jax import lax
from jax.experimental import pallas as pl
from jax.experimental.pallas import tpu as pltpu
from jax.sharding import PartitionSpec as P

GRID_W = 128


EPS = 1e-06
THETA = 10000.0


def turn_half(part, angle):
    quarter = part.shape[-1] // 2
    cos_table = jnp.cos(angle)[:, None, :]
    sin_table = jnp.sin(angle)[:, None, :]
    first_part = part[..., :quarter]
    second_part = part[..., quarter:]
    return jnp.concatenate(
        [
            first_part * cos_table - second_part * sin_table,
            first_part * sin_table + second_part * cos_table,
        ],
        axis=-1,
    )


def head_norm_rope(flat, gain, offset, head_count):
    tok_rows = flat.shape[0]
    head_size = flat.shape[1] // head_count
    heads = flat.astype(jnp.float32).reshape(tok_rows, head_count, head_size)
    heads = heads * lax.rsqrt(jnp.mean(heads * heads, axis=-1, keepdims=True) + EPS) * gain
    positions = offset + jnp.arange(tok_rows, dtype=jnp.int32)
    row_pos = (positions // GRID_W).astype(jnp.float32)
    col_pos = (positions % GRID_W).astype(jnp.float32)
    half_size = head_size // 2
    inv_freq = THETA ** (-jnp.arange(0, half_size, 2, dtype=jnp.float32) / half_size)
    turned = jnp.concatenate(
        [
            turn_half(heads[..., :half_size], row_pos[:, None] * inv_freq[None, :]),
            turn_half(heads[..., half_size:], col_pos[:, None] * inv_freq[None, :]),
        ],
        axis=-1,
    )
    return turned.reshape(tok_rows, head_count * head_size).astype(jnp.bfloat16)


def body(queries, keys, values, q_gain, k_gain, w_out, residual, norm_gain, w_gate, w_up, w_down):
    tok_rows = queries.shape[0]
    head_size = q_gain.shape[0]
    q_heads = queries.shape[1] // head_size
    kv_heads = keys.shape[1] // head_size
    q_group = q_heads // kv_heads
    offset = lax.axis_index("sp") * tok_rows
    q_rot = head_norm_rope(queries, q_gain, offset, q_heads)
    k_rot = head_norm_rope(keys, k_gain, offset, kv_heads)
    query_groups = q_rot.reshape(tok_rows, kv_heads, q_group, head_size)
    score_scale = head_size ** (-0.5)
    start_state = (
        jnp.full((kv_heads, q_group, tok_rows), -1e30, jnp.float32),
        jnp.zeros((kv_heads, q_group, tok_rows), jnp.float32),
        jnp.zeros((kv_heads, q_group, tok_rows, head_size), jnp.float32),
    )
    running = start_state
    key_piece = lax.all_gather(k_rot, "sp", axis=0, tiled=True)
    value_piece = lax.all_gather(values, "sp", axis=0, tiled=True)
    piece_len = key_piece.shape[0]
    block_len = math.gcd(piece_len, 512)
    blocks = piece_len // block_len
    key_blocks = key_piece.reshape(blocks, block_len, kv_heads, head_size)
    value_blocks = value_piece.reshape(blocks, block_len, kv_heads, head_size)

    def update(state, block_pair):
        prior_max, totals, accum = state
        key_block, value_block = block_pair
        scores = (
            jnp.einsum(
                "qhgd,khd->hgqk", query_groups, key_block, preferred_element_type=jnp.float32
            )
            * score_scale
        )
        new_max = jnp.maximum(prior_max, jnp.max(scores, axis=-1))
        weights = jnp.exp(scores - new_max[..., None])
        factor = jnp.exp(prior_max - new_max)
        totals = totals * factor + jnp.sum(weights, axis=-1)
        accum = accum * factor[..., None] + jnp.einsum(
            "hgqk,khd->hgqd",
            weights.astype(jnp.bfloat16),
            value_block,
            preferred_element_type=jnp.float32,
        )
        return ((new_max, totals, accum), None)

    running, unused = lax.scan(update, running, (key_blocks, value_blocks))
    final_max, totals, accum = running
    mixed = accum / totals[..., None]
    attn = (
        jnp.transpose(mixed, (2, 0, 1, 3))
        .reshape(tok_rows, q_heads * head_size)
        .astype(jnp.bfloat16)
    )
    own_rows = lax.all_to_all(attn, "tp", split_axis=0, concat_axis=1, tiled=True)
    columns = own_rows
    proj = jnp.dot(
        columns, lax.all_gather(w_out, "tp", axis=0, tiled=True), preferred_element_type=jnp.float32
    )
    mid = residual.astype(jnp.float32) + proj
    normed = (
        mid * lax.rsqrt(jnp.mean(mid * mid, axis=-1, keepdims=True) + EPS) * norm_gain
    ).astype(jnp.bfloat16)
    gathered = lax.all_gather(normed, "tp", axis=0, tiled=True)
    columns = gathered
    gate = jnp.dot(
        columns,
        lax.all_gather(w_gate, "sp", axis=0, tiled=True),
        preferred_element_type=jnp.float32,
    )
    up_part = jnp.dot(
        columns, lax.all_gather(w_up, "sp", axis=0, tiled=True), preferred_element_type=jnp.float32
    )
    hidden = (jax.nn.silu(gate) * up_part).astype(jnp.bfloat16)
    terms = jnp.dot(
        hidden, lax.all_gather(w_down, "sp", axis=1, tiled=True), preferred_element_type=jnp.float32
    )
    down = lax.psum_scatter(
        terms.astype(jnp.bfloat16), "tp", scatter_dimension=0, tiled=True
    ).astype(jnp.float32)
    return (mid + 0.5 * down).astype(jnp.bfloat16)


MESH = pl.DeviceIdType.MESH
BLOCK = 128


def line_of_chips(mesh):
    count = mesh.shape["sp"]
    try:
        places = [(tuple(d.coords), d.core_on_chip) for d in mesh.devices[:, 0].flat]
    except AttributeError:
        return None
    if count % 4 or count < 12 or mesh.shape["tp"] != 2:
        return None
    first = places[0][0]
    for at, (coords, core) in enumerate(places):
        chip = at // 2
        want = (first[0], first[1] + chip % 2, first[2] + chip // 2)
        if coords != want or core != at % 2:
            return None
    return count // 4


def message_count(n):
    events = 2 * (n - 1)
    keys = 2 * events + 6 * (events + 1)
    return keys + 27 * n + 1 + 2 * events + 8 * n


def turned_heads(head_size, x_ref, g_ref, cos_ref, sin_ref):
    x = x_ref[...].astype(jnp.float32)
    width = x.shape[1]
    lane = lax.broadcasted_iota(jnp.int32, (width, width), 0) // head_size
    other = lax.broadcasted_iota(jnp.int32, (width, width), 1) // head_size
    same = (lane == other).astype(jnp.float32)
    mean = jnp.dot(
        x * x, same, preferred_element_type=jnp.float32, precision=lax.Precision.HIGHEST
    ) * (1.0 / head_size)
    h = x * lax.rsqrt(mean + EPS) * jnp.concatenate([g_ref[...]] * (width // head_size), axis=1)
    quarter = head_size // 4
    repeats = width // cos_ref.shape[1]
    cos_table = jnp.concatenate([cos_ref[...]] * repeats, axis=1)
    sin_table = jnp.concatenate([sin_ref[...]] * repeats, axis=1)
    at = lax.broadcasted_iota(jnp.int32, x.shape, 1)
    is_first = (at // quarter) % 2 == 0
    ahead = pltpu.roll(h, width - quarter, 1)
    behind = pltpu.roll(h, quarter, 1)
    turned = h * cos_table + jnp.where(is_first, -ahead, behind) * sin_table
    return turned.astype(jnp.bfloat16)


def when(condition, action):
    if condition is None:
        action()
    else:
        pl.when(condition)(action)


def both(one, other):
    if one is None:
        return other
    if other is None:
        return one
    return jnp.logical_and(one, other)


def layer_kernel(
    n, head_size,
    raw_q, raw_k, raw_v, qg_ref, kg_ref, cos_ref, sin_ref, res_ref, gain_ref, wo_in, wg_in, wu_in, wd_in,
    out_ref,
    q_ref, kv_all, wg_all, wu_all, wd_all, wo_own, attn, context, proj_out, proj_in, mid, normed, hidden,
    part, leaving, line_in, own_sem, send_sem, recv_sem,
):
    sp = lax.axis_index("sp")
    tp = lax.axis_index("tp")
    core = lax.rem(sp, 2)
    y = lax.rem(lax.div(sp, 2), 2)
    z = lax.div(sp, 4)

    def device(zz, yy, cc):
        return (zz * 2 + yy) * 2 + cc

    def wrapped(zz):
        return lax.rem(zz + n, n)

    sibling = (device(z, y, 1 - core), tp)
    across = (device(z, 1 - y, core), tp)
    partner = (sp, 1 - tp)

    def level(zz):
        return (device(zz, y, core), tp)

    barrier = pltpu.get_barrier_semaphore()
    greeted = [sibling, across, partner] + [level(wrapped(z + d)) for d in range(1, n)]
    for target in greeted:
        pl.semaphore_signal(barrier, inc=1, device_id=target, device_id_type=MESH)
    pl.semaphore_wait(barrier, len(greeted))

    slots = {}
    sent = []

    def message(key, src, dst, target):
        slot = key
        if isinstance(key, tuple):
            slot = slots.setdefault(key, 3 * n + len(slots))
        return pltpu.make_async_remote_copy(
            src_ref=src, dst_ref=dst, send_sem=send_sem.at[slot], recv_sem=recv_sem.at[slot],
            device_id=target, device_id_type=MESH,
        )

    def send(key, condition, src, dst, target):
        def make():
            return message(key, src(), dst(), target)

        when(condition, lambda: make().start())
        sent.append((condition, make))

    def land(key, condition, piece):
        when(condition, lambda: message(key, piece(), piece(), partner).wait_recv())

    near = [z]
    for p in range(1, n):
        level_at = 0
        for zz in range(n):
            order = sorted(range(n), key=lambda other: (abs(other - zz), -abs(2 * other - n + 1)))
            level_at = jnp.where(z == zz, order[p], level_at)
        near.append(level_at)

    arrivals = [[(s, w) for w in range(2)] for s in range(n - 1)]
    events = [None] + [e for step in arrivals for e in step]
    room = (z <= n - 2, z >= 1)
    ahead = (level(z + 1), level(z - 1))

    def home(e):
        if e is None:
            return z
        return z - 1 - e[0] if e[1] == 0 else z + 1 + e[0]

    def real(e):
        if e is None:
            return None
        return z >= e[0] + 1 if e[1] == 0 else z <= n - 2 - e[0]

    def pass_on(name, e, src, dst):
        for w in range(2) if e is None else (e[1],):
            step = 0 if e is None else e[0] + 1
            if step <= n - 2:
                send((name, step, w), both(real(e), room[w]), src, dst, ahead[w])

    tok = raw_q.shape[0]
    kv_width = raw_k.shape[1]

    def kv_piece(j, zz, yy, cc):
        start = pl.multiple_of(device(zz, yy, cc) * tok, tok)
        return kv_all.at[pl.ds(start, tok), j * kv_width:(j + 1) * kv_width]

    def kv_serve(j, e):
        def dst():
            return kv_piece(j, home(e), y, core)

        if e is not None:
            land((("kv", j), e[0], e[1]), real(e), dst)
        src = (lambda: raw_v) if e is None and j == 1 else dst
        pass_on(("kv", j), e, src, dst)
        send(("kv y", j, e), real(e), src, dst, across)
        send(("kv core", j, e, 0), real(e), src, dst, sibling)

    def kv_cross(j, e):
        def piece():
            return kv_piece(j, home(e), 1 - y, core)

        land(("kv y", j, e), real(e), piece)
        send(("kv core", j, e, 1), real(e), piece, piece, sibling)

    def kv_finish(j, e):
        land(("kv core", j, e, 0), real(e), lambda: kv_piece(j, home(e), y, 1 - core))
        land(("kv core", j, e, 1), real(e), lambda: kv_piece(j, home(e), 1 - y, 1 - core))

    GATE, UP, DOWN = range(3)
    weights_in = (wg_in, wu_in, wd_in)
    rows, units = wg_in.shape
    lanes_down = wd_in.shape[1]
    slab = wg_all.shape[1]
    share = slab // BLOCK

    def first_block(zz, xx):
        return lax.div(zz * share + xx, 2)

    def unit_forms(zz, xx):
        if share % 2 == 0:
            return [(None, share // 2)]
        many = lax.rem(zz + xx, 2) == 1
        return [(jnp.logical_not(many), share // 2), (many, share // 2 + 1)]

    def weight_in(k, zz, count):
        span = pl.ds(pl.multiple_of(first_block(zz, tp) * BLOCK, BLOCK), count * BLOCK)
        return wd_in.at[span, :] if k == DOWN else weights_in[k].at[:, span]

    def weight(k, xx, zz, yy, cc, keeper, count):
        o = device(zz, yy, cc)
        before = xx * (first_block(keeper + 1, 0) - first_block(keeper, 0))
        units_of = pl.ds(pl.multiple_of(before * BLOCK, BLOCK), count * BLOCK)
        if k == DOWN:
            return wd_all.at[units_of, pl.ds(pl.multiple_of(o * lanes_down, lanes_down), lanes_down)]
        return (wg_all, wu_all)[k].at[pl.ds(pl.multiple_of(o * rows, rows), rows), units_of]

    def weight_line(k, p):
        zt = near[p]
        for condition, count in unit_forms(zt, tp):
            send(
                k * n + wrapped(zt - z), condition,
                functools.partial(weight_in, k, zt, count),
                functools.partial(weight, k, tp, z, y, core, zt, count), level(zt),
            )

    def by_x(k, p):
        return (p % 4 != 3, p % 2 == 0, p % 2 == 1)[k]

    def weight_move(k, p, xx, yy, way):
        target = {"x": partner, "y": across, "core": sibling}[way]
        corner = (xx is not tp, yy is not y)
        for condition, count in unit_forms(z, xx):
            dst = functools.partial(weight, k, xx, near[p], yy, core, z, count)
            src = dst
            if p == 0 and corner == (False, False):
                src = functools.partial(weight_in, k, z, count)
            send(("w", way, k, p, corner), condition, src, dst, target)

    other_x, other_y = 1 - tp, 1 - y

    def weight_take(key, k, p, xx, yy, cc):
        for condition, count in unit_forms(z, xx):
            land(key, condition, functools.partial(weight, k, xx, near[p], yy, cc, z, count))

    def weight_land(k, p, way, xx, yy):
        corner = (xx is not tp, yy is not y)
        seen = {"x": (not corner[0], corner[1]), "y": (corner[0], not corner[1])}[way]
        weight_take(("w", way, k, p, seen), k, p, xx, yy, core)

    def weight_arrive(k, p):
        weight_take(k * n + wrapped(z - near[p]), k, p, tp, y, core)

    def weight_serve(k, p):
        if p > 0:
            weight_arrive(k, p)
        weight_move(k, p, tp, y, "y")
        weight_move(k, p, tp, y, "x")
        weight_move(k, p, tp, y, "core")

    def cross_y(k, p):
        weight_land(k, p, "y", tp, other_y)
        if by_x(k, p):
            weight_move(k, p, tp, other_y, "x")
        weight_move(k, p, tp, other_y, "core")

    def cross_x(k, p):
        weight_land(k, p, "x", other_x, y)
        if not by_x(k, p):
            weight_move(k, p, other_x, y, "y")
        weight_move(k, p, other_x, y, "core")

    def cross_both(k, p):
        weight_land(k, p, "x" if by_x(k, p) else "y", other_x, other_y)
        weight_move(k, p, other_x, other_y, "core")

    def own_copy(k, count):
        return pltpu.make_async_copy(
            weight_in(k, z, count), weight(k, tp, z, y, core, z, count), own_sem.at[k]
        )

    def own_each(act):
        for k in range(3):
            for condition, count in unit_forms(z, tp):
                when(condition, lambda: act(own_copy(k, count)))

    own_wo = pltpu.make_async_copy(wo_in, wo_own, own_sem.at[3])

    def weight_finish(k, sides):
        for p in range(n):
            for xx in (tp, other_x):
                for yy in sides:
                    corner = (xx is not tp, yy is not y)
                    weight_take(("w", "core", k, p, corner), k, p, xx, yy, 1 - core)

    pairs, q_rows, lanes = q_ref.shape
    block = math.gcd(q_rows, 256)
    per_pair = q_rows // block

    def attend(at):
        pair, which = at // per_pair, at % per_pair
        span = slice(which * block, (which + 1) * block)
        q = q_ref[pair, span, :]
        k = kv_all[:, pair * lanes:(pair + 1) * lanes]
        v = kv_all[:, (pairs + pair) * lanes:(pairs + pair + 1) * lanes]
        scores = lax.dot_general(
            q, k, (((1,), (1,)), ((), ())), preferred_element_type=jnp.float32
        )
        weights = jnp.exp(scores - jnp.max(scores, axis=-1, keepdims=True))
        total = jnp.sum(weights, axis=-1, keepdims=True)
        mixed = jnp.dot(weights.astype(jnp.bfloat16), v, preferred_element_type=jnp.float32)
        attn[pair, span, :] = (mixed / total).astype(jnp.bfloat16)

    def assemble():
        group = q_rows // (2 * tok)
        pieces = []
        for pair in range(pairs):
            for side in range(2):
                for g in range(0, group, 2):
                    lower = attn[pair, pl.ds((side * group + g) * tok, tok), :].astype(jnp.float32)
                    upper = attn[pair, pl.ds((side * group + g + 1) * tok, tok), :].astype(jnp.float32)
                    if side == 1:
                        lower = pltpu.roll(lower, head_size, 1)
                    else:
                        upper = pltpu.roll(upper, head_size, 1)
                    lane = lax.broadcasted_iota(jnp.int32, lower.shape, 1)
                    pieces.append(jnp.where(lane < head_size, lower, upper).astype(jnp.bfloat16))
        context[...] = jnp.concatenate(pieces, axis=1)

    own_count, width = res_ref.shape
    rows_of = own_count // 2
    mine = pl.ds(pl.multiple_of(tp * own_count, own_count), own_count)
    theirs = pl.ds(pl.multiple_of((1 - tp) * own_count, own_count), own_count)

    def whole(zz):
        return pl.ds(pl.multiple_of(zz * own_count, own_count), own_count)

    def rows_at(zz, f):
        return pl.ds(pl.multiple_of((zz * 2 + f) * rows_of, rows_of), rows_of)

    wide = math.gcd(width, 512)

    def project():
        given = context[theirs, :]
        for at in range(0, width, wide):
            cols = slice(at, at + wide)
            proj_out[:, cols] = jnp.dot(
                given, wo_own[:, cols], preferred_element_type=jnp.float32
            ).astype(jnp.bfloat16)

    def project_own():
        held = context[mine, :]
        for at in range(0, width, wide):
            cols = slice(at, at + wide)
            mid[:, cols] = res_ref[:, cols].astype(jnp.float32) + jnp.dot(
                held, wo_own[:, cols], preferred_element_type=jnp.float32
            )

    def normalize():
        value = mid[...] + proj_in[...].astype(jnp.float32)
        mid[...] = value
        scale = lax.rsqrt(jnp.mean(value * value, axis=-1, keepdims=True) + EPS)
        normed[whole(z), :] = (value * scale * gain_ref[...]).astype(jnp.bfloat16)

    def rows_serve(f, e):
        def piece():
            return normed.at[rows_at(home(e), f), :]

        if e is not None:
            land((("rows", f), e[0], e[1]), real(e), piece)
        pass_on(("rows", f), e, piece, piece)

    half_rows = normed.shape[0] // 2
    tile = 2 * lanes_down

    def feed(h):
        span = pl.ds(pl.multiple_of(h * half_rows, half_rows), half_rows)

        def some(cols):
            x = normed[span, :]
            gate = jnp.dot(x, wg_all[:, cols], preferred_element_type=jnp.float32)
            up = jnp.dot(x, wu_all[:, cols], preferred_element_type=jnp.float32)
            hidden[span, cols] = (gate / (1.0 + jnp.exp(-gate)) * up).astype(jnp.bfloat16)

        @pl.loop(0, slab // tile)
        def _(at):
            some(pl.ds(pl.multiple_of(at * tile, tile), tile))

        if slab % tile:
            some(slice(slab - slab % tile, slab))

    groups = 4
    cols_of = width // groups

    def result_columns(g, at):
        zs = g % 2 * (n // 2) + at
        start = (zs * 4 + 2 * (y, other_y)[g // 2]) * lanes_down
        return pl.ds(pl.multiple_of(start, tile), tile)

    def lower(g):
        @pl.loop(0, n // 2)
        def _(at):
            cols = pl.ds(pl.multiple_of(g * cols_of + at * tile, tile), tile)
            part[:, cols] = jnp.dot(
                hidden[...], wd_all[:, result_columns(g, at)], preferred_element_type=jnp.float32
            )

    def columns(g):
        return slice(g * cols_of, (g + 1) * cols_of)

    def add(zz, f, ref):
        part[whole(zz), columns(f)] = part[whole(zz), columns(f)] + ref[...].astype(jnp.float32)

    def sum_send(f, w, d):
        zz = z + d if w == 0 else z - d
        inside = z <= n - 1 - d if w == 0 else z >= d
        if d < n - 1:
            def take():
                message(("sum", f, w, d + 1), line_in.at[f, w, d], line_in.at[f, w, d], partner).wait_recv()
                add(zz, f, line_in.at[f, w, d])

            when(both(inside, room[1 - w]), take)

        def put():
            leaving[whole(zz), columns(f)] = part[whole(zz), columns(f)].astype(jnp.bfloat16)

        when(inside, put)
        send(
            ("sum", f, w, d), inside,
            lambda: leaving.at[whole(zz), columns(f)], lambda: line_in.at[f, w, d - 1], ahead[w],
        )

    def sum_finish(f):
        for w in range(2):
            def take():
                message(("sum", f, w, 1), line_in.at[f, w, 0], line_in.at[f, w, 0], partner).wait_recv()
                add(z, f, line_in.at[f, w, 0])

            when(room[1 - w], take)
        for at in range(n // 2):
            cols = result_columns(f, at)
            start = f * cols_of + at * tile
            down = part[whole(z), start:start + tile]
            out_ref[:, cols] = (mid[:, cols] + 0.5 * down).astype(jnp.bfloat16)

    own_each(lambda copy: copy.start())
    own_wo.start()
    kv_serve(1, None)
    own_rows = pl.ds(pl.multiple_of(sp * tok, tok), tok)
    kv_all[own_rows, :kv_width] = turned_heads(head_size, raw_k, kg_ref, cos_ref, sin_ref)
    kv_all[own_rows, kv_width:] = raw_v[...]
    for k in range(3):
        weight_move(k, 0, tp, y, "x")
        weight_move(k, 0, tp, y, "core")
    kv_serve(0, None)
    weight_move(GATE, 0, tp, y, "y")
    for p in range(1, n):
        weight_line(GATE, p)
    turned = turned_heads(head_size, raw_q, qg_ref, cos_ref, sin_ref).astype(jnp.float32)
    turned = turned * head_size ** (-0.5)
    group = q_rows // (2 * tok)
    for at in range(raw_q.shape[1] // lanes):
        together = turned[:, at * lanes:(at + 1) * lanes]
        swapped = pltpu.roll(together, head_size, 1)
        low = lax.broadcasted_iota(jnp.int32, together.shape, 1) < head_size
        key_head, g = 2 * at // group, 2 * at % group
        pair, side = key_head // 2, key_head % 2
        for extra in range(2):
            source = together if extra == side else swapped
            kept_lanes = jnp.where(low if side == 0 else jnp.logical_not(low), source, 0.0)
            first = (side * group + g + extra) * tok
            q_ref[pair, first:first + tok, :] = kept_lanes.astype(jnp.bfloat16)

    def all_lines(k):
        for p in range(1, n):
            weight_line(k, p)

    serve = [(k, d) for k in range(3) for d in range(1, n)]
    over_x = [(k, d) for k in range(3) for d in range(n)]
    over_y, over_both = list(over_x), list(over_x)
    queues = {"s": (weight_serve, serve), "x": (cross_x, over_x), "y": (cross_y, over_y), "b": (cross_both, over_both), "l": (all_lines, [(UP,), (DOWN,)])}

    def work(plan):
        for letter in plan:
            task, queue = queues[letter]
            if queue:
                task(*queue.pop(0))

    crossing = [None]
    for at, step in enumerate(arrivals):
        for j in (1, 0):
            for e in step:
                kv_serve(j, e)
        work(("", "xys", "l")[max(0, at - n + 4)])
        for j in (1, 0):
            for e in crossing:
                kv_cross(j, e)
        crossing = step
    work("s")
    for j in (1, 0):
        for e in crossing:
            kv_cross(j, e)
    work("s")
    weight_move(UP, 0, tp, y, "y")
    for j in (1, 0):
        for e in events:
            kv_finish(j, e)
    plans = ["xy", "", "", "xy", "", "l"]
    for at in range(pairs * per_pair):
        attend(at)
        work(plans[at % len(plans)])
    assemble()
    own_wo.wait()
    project()
    send(("proj",), None, lambda: proj_out, lambda: proj_in, partner)
    project_own()
    weight_move(DOWN, 0, tp, y, "y")
    work("sxys")
    land(("proj",), None, lambda: proj_in)
    normalize()
    for f in range(2):
        rows_serve(f, None)

    def rows_step(at):
        for f in range(2):
            for e in arrivals[at]:
                rows_serve(f, e)

    work("xysxyxysxyxyss")
    rows_step(0)
    while over_both[0][0] < DOWN:
        work("b")
    own_each(lambda copy: copy.wait())
    weight_finish(GATE, (y, other_y))
    weight_finish(UP, (y, other_y))
    upper_half = lax.div(z, n // 2)
    feed(upper_half)
    for at in range(1, n - 1):
        work("xy")
        rows_step(at)
        work("xy")
    work("xy" * len(over_x))
    feed(1 - upper_half)
    weight_finish(DOWN, (y,))
    for two in ((0, 1), (2, 3)):
        if two[0]:
            work("b" * len(over_both))
            weight_finish(DOWN, (other_y,))
        for g in two:
            lower(g)
            for w in range(2):
                sum_send(g, w, n - 1)
        work("y" * len(over_y))
        for d in range(n - 2, 0, -1):
            for g in two:
                for w in range(2):
                    sum_send(g, w, d)
    for g in range(groups):
        sum_finish(g)
    for condition, make in sent:
        when(condition, lambda: make().wait_send())
    assert len(slots) <= send_sem.shape[0]


def fast_body(n, queries, keys, values, q_gain, k_gain, w_out, residual, norm_gain, w_gate, w_up, w_down):
    tok_rows = queries.shape[0]
    head_size = q_gain.shape[0]
    q_heads = queries.shape[1] // head_size
    kv_heads = keys.shape[1] // head_size
    q_group = q_heads // kv_heads
    if 2 * w_gate.shape[1] % (n * BLOCK) or n % 2:
        return body(
            queries, keys, values, q_gain, k_gain, w_out, residual, norm_gain, w_gate, w_up, w_down
        )
    n_sp = 4 * n
    positions = lax.axis_index("sp") * tok_rows + jnp.arange(tok_rows, dtype=jnp.int32)
    half_size = head_size // 2
    inv_freq = THETA ** (-jnp.arange(0, half_size, 2, dtype=jnp.float32) / half_size)
    row_angle = (positions // GRID_W).astype(jnp.float32)[:, None] * inv_freq[None, :]
    col_angle = (positions % GRID_W).astype(jnp.float32)[:, None] * inv_freq[None, :]
    angle = jnp.concatenate([row_angle, row_angle, col_angle, col_angle] * 2, axis=1)
    cos_table, sin_table = jnp.cos(angle), jnp.sin(angle)
    pairs = kv_heads // 2
    padded = (pairs, 2 * q_group * tok_rows, 2 * head_size)
    kv_width = keys.shape[1] + values.shape[1]
    tokens = n_sp * tok_rows
    any_space = pl.BlockSpec(memory_space=pl.ANY)
    vmem = pl.BlockSpec(memory_space=pltpu.VMEM)
    own_count, width = residual.shape
    depth_in, units = w_gate.shape
    lanes_down = w_down.shape[1]
    slab = 2 * units // n
    group_rows = n * own_count
    bf16, f32 = jnp.bfloat16, jnp.float32
    return pl.pallas_call(
        functools.partial(layer_kernel, n, head_size),
        out_shape=jax.ShapeDtypeStruct(residual.shape, bf16),
        in_specs=[vmem] * 9 + [any_space] * 4,
        out_specs=vmem,
        scratch_shapes=[
            pltpu.VMEM(padded, bf16),
            pltpu.VMEM((tokens, kv_width), bf16),
            pltpu.VMEM((n_sp * depth_in, slab), bf16),
            pltpu.VMEM((n_sp * depth_in, slab), bf16),
            pltpu.VMEM((slab, n_sp * lanes_down), bf16),
            pltpu.VMEM(w_out.shape, bf16),
            pltpu.VMEM(padded, bf16),
            pltpu.VMEM(queries.shape, bf16),
            pltpu.VMEM((own_count, width), bf16),
            pltpu.VMEM((own_count, width), bf16),
            pltpu.VMEM((own_count, width), f32),
            pltpu.VMEM((group_rows, width), bf16),
            pltpu.VMEM((group_rows, slab), bf16),
            pltpu.VMEM((group_rows, width), f32),
            pltpu.VMEM((group_rows, width), bf16),
            pltpu.VMEM((4, 2, n - 1, own_count, width // 4), bf16),
            pltpu.SemaphoreType.DMA((4,)),
            pltpu.SemaphoreType.DMA((message_count(n),)),
            pltpu.SemaphoreType.DMA((message_count(n),)),
        ],
        compiler_params=pltpu.CompilerParams(
            collective_id=0, has_side_effects=True, vmem_limit_bytes=63 * 1024 * 1024
        ),
        name="layer",
    )(
        queries, keys, values, q_gain[None, :], k_gain[None, :], cos_table, sin_table,
        residual, norm_gain[None, :], w_out, w_gate, w_up, w_down)


def solution(mesh):
    n = line_of_chips(mesh)
    inner = body if n is None else functools.partial(fast_body, n)
    return jax.shard_map(
        inner,
        mesh=mesh,
        in_specs=(
            P("sp", "tp"),
            P("sp", "tp"),
            P("sp", "tp"),
            P(),
            P(),
            P("tp", None),
            P(("sp", "tp"), None),
            P(),
            P("sp", "tp"),
            P("sp", "tp"),
            P("tp", "sp"),
        ),
        out_specs=P(("sp", "tp"), None),
        check_vma=False,
    )
```

```python
import functools
import math

import jax
import jax.numpy as jnp
import numpy as np
from jax import lax
from jax.experimental import pallas as pl
from jax.experimental.pallas import tpu as pltpu
from jax.sharding import PartitionSpec as P

GRID_W = 128


EPS = 1e-06
THETA = 10000.0


def turn_half(part, angle):
    quarter = part.shape[-1] // 2
    cos_table = jnp.cos(angle)[:, None, :]
    sin_table = jnp.sin(angle)[:, None, :]
    first_part = part[..., :quarter]
    second_part = part[..., quarter:]
    return jnp.concatenate(
        [
            first_part * cos_table - second_part * sin_table,
            first_part * sin_table + second_part * cos_table,
        ],
        axis=-1,
    )


def head_norm_rope(flat, gain, offset, head_count):
    tok_rows = flat.shape[0]
    head_size = flat.shape[1] // head_count
    heads = flat.astype(jnp.float32).reshape(tok_rows, head_count, head_size)
    heads = heads * lax.rsqrt(jnp.mean(heads * heads, axis=-1, keepdims=True) + EPS) * gain
    positions = offset + jnp.arange(tok_rows, dtype=jnp.int32)
    row_pos = (positions // GRID_W).astype(jnp.float32)
    col_pos = (positions % GRID_W).astype(jnp.float32)
    half_size = head_size // 2
    inv_freq = THETA ** (-jnp.arange(0, half_size, 2, dtype=jnp.float32) / half_size)
    turned = jnp.concatenate(
        [
            turn_half(heads[..., :half_size], row_pos[:, None] * inv_freq[None, :]),
            turn_half(heads[..., half_size:], col_pos[:, None] * inv_freq[None, :]),
        ],
        axis=-1,
    )
    return turned.reshape(tok_rows, head_count * head_size).astype(jnp.bfloat16)


def body(queries, keys, values, q_gain, k_gain, w_out, residual, norm_gain, w_gate, w_up, w_down):
    tok_rows = queries.shape[0]
    head_size = q_gain.shape[0]
    q_heads = queries.shape[1] // head_size
    kv_heads = keys.shape[1] // head_size
    q_group = q_heads // kv_heads
    offset = lax.axis_index("sp") * tok_rows
    q_rot = head_norm_rope(queries, q_gain, offset, q_heads)
    k_rot = head_norm_rope(keys, k_gain, offset, kv_heads)
    query_groups = q_rot.reshape(tok_rows, kv_heads, q_group, head_size)
    score_scale = head_size ** (-0.5)
    start_state = (
        jnp.full((kv_heads, q_group, tok_rows), -1e30, jnp.float32),
        jnp.zeros((kv_heads, q_group, tok_rows), jnp.float32),
        jnp.zeros((kv_heads, q_group, tok_rows, head_size), jnp.float32),
    )
    running = start_state
    key_piece = lax.all_gather(k_rot, "sp", axis=0, tiled=True)
    value_piece = lax.all_gather(values, "sp", axis=0, tiled=True)
    piece_len = key_piece.shape[0]
    block_len = math.gcd(piece_len, 512)
    blocks = piece_len // block_len
    key_blocks = key_piece.reshape(blocks, block_len, kv_heads, head_size)
    value_blocks = value_piece.reshape(blocks, block_len, kv_heads, head_size)

    def update(state, block_pair):
        prior_max, totals, accum = state
        key_block, value_block = block_pair
        scores = (
            jnp.einsum(
                "qhgd,khd->hgqk", query_groups, key_block, preferred_element_type=jnp.float32
            )
            * score_scale
        )
        new_max = jnp.maximum(prior_max, jnp.max(scores, axis=-1))
        weights = jnp.exp(scores - new_max[..., None])
        factor = jnp.exp(prior_max - new_max)
        totals = totals * factor + jnp.sum(weights, axis=-1)
        accum = accum * factor[..., None] + jnp.einsum(
            "hgqk,khd->hgqd",
            weights.astype(jnp.bfloat16),
            value_block,
            preferred_element_type=jnp.float32,
        )
        return ((new_max, totals, accum), None)

    running, unused = lax.scan(update, running, (key_blocks, value_blocks))
    final_max, totals, accum = running
    mixed = accum / totals[..., None]
    attn = (
        jnp.transpose(mixed, (2, 0, 1, 3))
        .reshape(tok_rows, q_heads * head_size)
        .astype(jnp.bfloat16)
    )
    own_rows = lax.all_to_all(attn, "tp", split_axis=0, concat_axis=1, tiled=True)
    columns = own_rows
    proj = jnp.dot(
        columns, lax.all_gather(w_out, "tp", axis=0, tiled=True), preferred_element_type=jnp.float32
    )
    mid = residual.astype(jnp.float32) + proj
    normed = (
        mid * lax.rsqrt(jnp.mean(mid * mid, axis=-1, keepdims=True) + EPS) * norm_gain
    ).astype(jnp.bfloat16)
    gathered = lax.all_gather(normed, "tp", axis=0, tiled=True)
    columns = gathered
    gate = jnp.dot(
        columns,
        lax.all_gather(w_gate, "sp", axis=0, tiled=True),
        preferred_element_type=jnp.float32,
    )
    up_part = jnp.dot(
        columns, lax.all_gather(w_up, "sp", axis=0, tiled=True), preferred_element_type=jnp.float32
    )
    hidden = (jax.nn.silu(gate) * up_part).astype(jnp.bfloat16)
    terms = jnp.dot(
        hidden, lax.all_gather(w_down, "sp", axis=1, tiled=True), preferred_element_type=jnp.float32
    )
    down = lax.psum_scatter(
        terms.astype(jnp.bfloat16), "tp", scatter_dimension=0, tiled=True
    ).astype(jnp.float32)
    return (mid + 0.5 * down).astype(jnp.bfloat16)


MESH = pl.DeviceIdType.MESH
BLOCK = 128


def line_of_chips(mesh):
    count = mesh.shape["sp"]
    try:
        places = [(tuple(d.coords), d.core_on_chip) for d in mesh.devices[:, 0].flat]
    except AttributeError:
        return None
    if count % 4 or count < 12 or mesh.shape["tp"] != 2:
        return None
    first = places[0][0]
    for at, (coords, core) in enumerate(places):
        chip = at // 2
        want = (first[0], first[1] + chip % 2, first[2] + chip // 2)
        if coords != want or core != at % 2:
            return None
    return count // 4


def message_count(n):
    events = 2 * (n - 1)
    keys_and_values = 2 * events + 2 * (events + 1) + 1
    weights = 3 * n + 9 * n + 4
    return keys_and_values + weights + 1 + 2 * events + 8 * (n - 1)


def turned_heads(head_size, x_ref, g_ref, cos_ref, sin_ref):
    x = x_ref[...].astype(jnp.float32)
    width = x.shape[1]
    lane = lax.broadcasted_iota(jnp.int32, (width, width), 0) // head_size
    other = lax.broadcasted_iota(jnp.int32, (width, width), 1) // head_size
    same = (lane == other).astype(jnp.float32)
    mean = jnp.dot(
        x * x, same, preferred_element_type=jnp.float32, precision=lax.Precision.HIGHEST
    ) * (1.0 / head_size)
    h = x * lax.rsqrt(mean + EPS) * jnp.concatenate([g_ref[...]] * (width // head_size), axis=1)
    quarter = head_size // 4
    repeats = width // cos_ref.shape[1]
    cos_table = jnp.concatenate([cos_ref[...]] * repeats, axis=1)
    sin_table = jnp.concatenate([sin_ref[...]] * repeats, axis=1)
    at = lax.broadcasted_iota(jnp.int32, x.shape, 1)
    is_first = (at // quarter) % 2 == 0
    ahead = pltpu.roll(h, width - quarter, 1)
    behind = pltpu.roll(h, quarter, 1)
    turned = h * cos_table + jnp.where(is_first, -ahead, behind) * sin_table
    return turned.astype(jnp.bfloat16)


def when(condition, action):
    if condition is None:
        action()
    else:
        pl.when(condition)(action)


def both(one, other):
    if one is None:
        return other
    if other is None:
        return one
    return jnp.logical_and(one, other)


def layer_kernel(
    n, head_size,
    raw_q, raw_k, raw_v, qg_ref, kg_ref, freq_ref, res_ref, gain_ref, wo_in, wg_in, wu_in, wd_in,
    out_ref,
    q_ref, kv_all, wg_all, wu_all, wd_all, wo_own, attn, context, proj_out, proj_in, mid, normed, hidden,
    part, leaving, line_in, out_own, cos_ref, sin_ref, own_sem, out_sem, send_sem, recv_sem,
):
    sp = lax.axis_index("sp")
    tp = lax.axis_index("tp")
    core = lax.rem(sp, 2)
    y = lax.rem(lax.div(sp, 2), 2)
    z = lax.div(sp, 4)

    def device(zz, yy, cc):
        return (zz * 2 + yy) * 2 + cc

    def wrapped(zz):
        return lax.rem(zz + n, n)

    sibling = (device(z, y, 1 - core), tp)
    across = (device(z, 1 - y, core), tp)
    partner = (sp, 1 - tp)

    def level(zz):
        return (device(zz, y, core), tp)

    barrier = pltpu.get_barrier_semaphore()
    greeted = [sibling, across, partner] + [level(wrapped(z + d)) for d in range(1, n)]
    for target in greeted:
        pl.semaphore_signal(barrier, inc=1, device_id=target, device_id_type=MESH)
    pl.semaphore_wait(barrier, len(greeted))

    slots = {}
    sent = []

    def message(key, src, dst, target):
        slot = key
        if isinstance(key, tuple):
            slot = slots.setdefault(key, 3 * n + len(slots))
        return pltpu.make_async_remote_copy(
            src_ref=src, dst_ref=dst, send_sem=send_sem.at[0], recv_sem=recv_sem.at[slot],
            device_id=target, device_id_type=MESH,
        )

    def send(key, condition, src, dst, target):
        def make():
            return message(key, src(), dst(), target)

        when(condition, lambda: make().start())
        sent.append((condition, make))

    def land(key, condition, piece):
        when(condition, lambda: message(key, piece(), piece(), partner).wait_recv())

    near = [z]
    for p in range(1, n):
        level_at = 0
        for zz in range(n):
            order = sorted(range(n), key=lambda other: (abs(other - zz), -abs(2 * other - n + 1)))
            level_at = jnp.where(z == zz, order[p], level_at)
        near.append(level_at)

    arrivals = [[(s, w) for w in range(2)] for s in range(n - 1)]
    events = [None] + [e for step in arrivals for e in step]
    room = (z <= n - 2, z >= 1)
    ahead = (level(z + 1), level(z - 1))

    def home(e):
        if e is None:
            return z
        return z - 1 - e[0] if e[1] == 0 else z + 1 + e[0]

    def real(e):
        if e is None:
            return None
        return z >= e[0] + 1 if e[1] == 0 else z <= n - 2 - e[0]

    def pass_on(name, e, src, dst):
        for w in range(2) if e is None else (e[1],):
            step = 0 if e is None else e[0] + 1
            if step <= n - 2:
                send((name, step, w), both(real(e), room[w]), src, dst, ahead[w])

    tok = raw_q.shape[0]
    kv_width = raw_k.shape[1]

    def kv_piece(j, zz, yy, cc):
        start = pl.multiple_of(device(zz, yy, cc) * tok, tok)
        return kv_all.at[pl.ds(start, tok), j * kv_width:(j + 1) * kv_width]

    def kv_serve(j, e):
        def dst():
            return kv_piece(j, home(e), y, core)

        if e is not None:
            land((("kv", j), e[0], e[1]), real(e), dst)
        src = (lambda: raw_v) if e is None and j == 1 else dst
        pass_on(("kv", j), e, src, dst)
        send(("kv y", j, e), real(e), src, dst, across)
        send(("kv core",), real(e), src, dst, sibling)

    def kv_cross(j, e):
        def piece():
            return kv_piece(j, home(e), 1 - y, core)

        land(("kv y", j, e), real(e), piece)
        send(("kv core",), real(e), piece, piece, sibling)

    def kv_finish():
        land(("kv core",), None, lambda: kv_all.at[:kv_all.shape[0] // 2, :])

    GATE, UP, DOWN = range(3)
    weights_in = (wg_in, wu_in, wd_in)
    rows, units = wg_in.shape
    lanes_down = wd_in.shape[1]
    slab = wg_all.shape[1]
    share = slab // BLOCK

    def first_block(zz, xx):
        return lax.div(zz * share + xx, 2)

    def unit_forms(zz, xx):
        if share % 2 == 0:
            return [(None, share // 2)]
        many = lax.rem(zz + xx, 2) == 1
        return [(jnp.logical_not(many), share // 2), (many, share // 2 + 1)]

    def weight_in(k, zz, count):
        span = pl.ds(pl.multiple_of(first_block(zz, tp) * BLOCK, BLOCK), count * BLOCK)
        return wd_in.at[span, :] if k == DOWN else weights_in[k].at[:, span]

    def weight(k, xx, zz, yy, cc, keeper, count):
        o = device(zz, yy, cc)
        before = xx * (first_block(keeper + 1, 0) - first_block(keeper, 0))
        units_of = pl.ds(pl.multiple_of(before * BLOCK, BLOCK), count * BLOCK)
        if k == DOWN:
            return wd_all.at[units_of, pl.ds(pl.multiple_of(o * lanes_down, lanes_down), lanes_down)]
        return (wg_all, wu_all)[k].at[pl.ds(pl.multiple_of(o * rows, rows), rows), units_of]

    def weight_line(k, p):
        zt = near[p]
        for condition, count in unit_forms(zt, tp):
            send(
                k * n + wrapped(zt - z), condition,
                functools.partial(weight_in, k, zt, count),
                functools.partial(weight, k, tp, z, y, core, zt, count), level(zt),
            )

    def by_x(k, p):
        return (p % 4 != 3, p % 2 == 0, p % 2 == 1)[k]

    def weight_move(k, p, xx, yy, way):
        target = {"x": partner, "y": across, "core": sibling}[way]
        corner = (xx is not tp, yy is not y)
        for condition, count in unit_forms(z, xx):
            dst = functools.partial(weight, k, xx, near[p], yy, core, z, count)
            src = dst
            if p == 0 and corner == (False, False):
                src = functools.partial(weight_in, k, z, count)
            key = ("w", way, k, p, corner)
            if way == "core":
                key = ("w", way, k, k == DOWN and corner[1])
            send(key, condition, src, dst, target)

    other_x, other_y = 1 - tp, 1 - y

    def weight_take(key, k, p, xx, yy, cc):
        for condition, count in unit_forms(z, xx):
            land(key, condition, functools.partial(weight, k, xx, near[p], yy, cc, z, count))

    def weight_land(k, p, way, xx, yy):
        corner = (xx is not tp, yy is not y)
        seen = {"x": (not corner[0], corner[1]), "y": (corner[0], not corner[1])}[way]
        weight_take(("w", way, k, p, seen), k, p, xx, yy, core)

    def weight_arrive(k, p):
        weight_take(k * n + wrapped(z - near[p]), k, p, tp, y, core)

    def weight_serve(k, p):
        if p > 0:
            weight_arrive(k, p)
        weight_move(k, p, tp, y, "y")
        weight_move(k, p, tp, y, "x")
        weight_move(k, p, tp, y, "core")

    def cross_y(k, p):
        weight_land(k, p, "y", tp, other_y)
        if by_x(k, p):
            weight_move(k, p, tp, other_y, "x")
        weight_move(k, p, tp, other_y, "core")

    def cross_x(k, p):
        weight_land(k, p, "x", other_x, y)
        if not by_x(k, p):
            weight_move(k, p, other_x, y, "y")
        weight_move(k, p, other_x, y, "core")

    def cross_both(k, p):
        weight_land(k, p, "x" if by_x(k, p) else "y", other_x, other_y)
        weight_move(k, p, other_x, other_y, "core")

    def own_copy(k, count):
        return pltpu.make_async_copy(
            weight_in(k, z, count), weight(k, tp, z, y, core, z, count), own_sem.at[k]
        )

    def own_each(act):
        for k in range(3):
            for condition, count in unit_forms(z, tp):
                when(condition, lambda: act(own_copy(k, count)))

    own_wo = pltpu.make_async_copy(wo_in, wo_own, own_sem.at[3])

    def weight_finish(k, second=False):
        def bulk():
            if k == DOWN:
                return wd_all.at[:, :wd_all.shape[1] // 4]
            ref = (wg_all, wu_all)[k]
            return ref.at[:ref.shape[0] // 2, :]

        land(("w", "core", k, second), None, bulk)

    pairs, q_rows, lanes = q_ref.shape
    block = math.gcd(q_rows, 256)
    per_pair = q_rows // block

    def attend(at):
        pair, which = at // per_pair, at % per_pair
        span = slice(which * block, (which + 1) * block)
        q = q_ref[pair, span, :]
        k = kv_all[:, pair * lanes:(pair + 1) * lanes]
        v = kv_all[:, (pairs + pair) * lanes:(pairs + pair + 1) * lanes]
        scores = lax.dot_general(
            q, k, (((1,), (1,)), ((), ())), preferred_element_type=jnp.float32
        )
        weights = jnp.exp(scores - jnp.max(scores, axis=-1, keepdims=True))
        total = jnp.sum(weights, axis=-1, keepdims=True)
        mixed = jnp.dot(weights.astype(jnp.bfloat16), v, preferred_element_type=jnp.float32)
        attn[pair, span, :] = (mixed / total).astype(jnp.bfloat16)

    def assemble():
        group = q_rows // (2 * tok)
        pieces = []
        for pair in range(pairs):
            for side in range(2):
                for g in range(0, group, 2):
                    lower = attn[pair, pl.ds((side * group + g) * tok, tok), :].astype(jnp.float32)
                    upper = attn[pair, pl.ds((side * group + g + 1) * tok, tok), :].astype(jnp.float32)
                    if side == 1:
                        lower = pltpu.roll(lower, head_size, 1)
                    else:
                        upper = pltpu.roll(upper, head_size, 1)
                    lane = lax.broadcasted_iota(jnp.int32, lower.shape, 1)
                    pieces.append(jnp.where(lane < head_size, lower, upper).astype(jnp.bfloat16))
        context[...] = jnp.concatenate(pieces, axis=1)

    own_count, width = res_ref.shape
    rows_of = own_count // 2
    mine = pl.ds(pl.multiple_of(tp * own_count, own_count), own_count)
    theirs = pl.ds(pl.multiple_of((1 - tp) * own_count, own_count), own_count)

    def whole(zz):
        return pl.ds(pl.multiple_of(zz * own_count, own_count), own_count)

    def rows_at(zz, f):
        return pl.ds(pl.multiple_of((zz * 2 + f) * rows_of, rows_of), rows_of)

    wide = math.gcd(width, 512)

    def project():
        given = context[theirs, :]
        for at in range(0, width, wide):
            cols = slice(at, at + wide)
            proj_out[:, cols] = jnp.dot(
                given, wo_own[:, cols], preferred_element_type=jnp.float32
            ).astype(jnp.bfloat16)

    def project_own():
        held = context[mine, :]
        for at in range(0, width, wide):
            cols = slice(at, at + wide)
            mid[:, cols] = res_ref[:, cols].astype(jnp.float32) + jnp.dot(
                held, wo_own[:, cols], preferred_element_type=jnp.float32
            )

    def normalize():
        value = mid[...] + proj_in[...].astype(jnp.float32)
        mid[...] = value
        scale = lax.rsqrt(jnp.mean(value * value, axis=-1, keepdims=True) + EPS)
        normed[whole(z), :] = (value * scale * gain_ref[...]).astype(jnp.bfloat16)

    def rows_serve(f, e):
        def piece():
            return normed.at[rows_at(home(e), f), :]

        if e is not None:
            land((("rows", f), e[0], e[1]), real(e), piece)
        pass_on(("rows", f), e, piece, piece)

    half_rows = normed.shape[0] // 2
    tile = 2 * lanes_down

    def feed(h):
        span = pl.ds(pl.multiple_of(h * half_rows, half_rows), half_rows)

        def some(cols):
            x = normed[span, :]
            gate = jnp.dot(x, wg_all[:, cols], preferred_element_type=jnp.float32)
            up = jnp.dot(x, wu_all[:, cols], preferred_element_type=jnp.float32)
            hidden[span, cols] = (gate / (1.0 + jnp.exp(-gate)) * up).astype(jnp.bfloat16)

        @pl.loop(0, slab // tile)
        def _(at):
            some(pl.ds(pl.multiple_of(at * tile, tile), tile))

        if slab % tile:
            some(slice(slab - slab % tile, slab))

    groups = 4
    cols_of = width // groups

    def result_columns(g, at):
        zs = g % 2 * (n // 2) + at
        start = (zs * 4 + 2 * (y, other_y)[g // 2]) * lanes_down
        return pl.ds(pl.multiple_of(start, tile), tile)

    def lower(g):
        @pl.loop(0, n // 2)
        def _(at):
            cols = pl.ds(pl.multiple_of(g * cols_of + at * tile, tile), tile)
            part[:, cols] = jnp.dot(
                hidden[...], wd_all[:, result_columns(g, at)], preferred_element_type=jnp.float32
            )

    def columns(g):
        return slice(g * cols_of, (g + 1) * cols_of)

    def add(zz, f, ref):
        part[whole(zz), columns(f)] = part[whole(zz), columns(f)] + ref[...].astype(jnp.float32)

    def sum_step(f, d):
        for w in range(2):
            sum_send(f, w, d, z <= n - 1 - d if w == 0 else z >= d)

    def sum_send(f, w, d, inside):
        zz = z + d if w == 0 else z - d
        if d < n - 1:
            def take():
                message(("sum", f, w, d + 1), line_in.at[f, w, d], line_in.at[f, w, d], partner).wait_recv()
                add(zz, f, line_in.at[f, w, d])

            when(both(inside, room[1 - w]), take)

        def put():
            leaving[whole(zz), columns(f)] = part[whole(zz), columns(f)].astype(jnp.bfloat16)

        when(inside, put)
        send(
            ("sum", f, w, d), inside,
            lambda: leaving.at[whole(zz), columns(f)], lambda: line_in.at[f, w, d - 1], ahead[w],
        )

    def out_copy(g, at):
        cols = result_columns(g, at)
        return pltpu.make_async_copy(
            out_own.at[:, cols], out_ref.at[:, cols], out_sem.at[g * (n // 2) + at]
        )

    def sum_finish(f):
        for w in range(2):
            def take():
                message(("sum", f, w, 1), line_in.at[f, w, 0], line_in.at[f, w, 0], partner).wait_recv()
                add(z, f, line_in.at[f, w, 0])

            when(room[1 - w], take)
        for at in range(n // 2):
            cols = result_columns(f, at)
            start = f * cols_of + at * tile
            down = part[whole(z), start:start + tile]
            out_own[:, cols] = (mid[:, cols] + 0.5 * down).astype(jnp.bfloat16)
            out_copy(f, at).start()

    own_each(lambda copy: copy.start())
    own_wo.start()
    kv_serve(1, None)
    own_rows = pl.ds(pl.multiple_of(sp * tok, tok), tok)
    at_row = (sp * tok + lax.broadcasted_iota(jnp.int32, cos_ref.shape, 0)).astype(jnp.float32)
    grid_row = jnp.floor(at_row * (1.0 / GRID_W))
    lane = lax.broadcasted_iota(jnp.int32, cos_ref.shape, 1)
    by_row = jnp.bitwise_and(lane, head_size - 1) < head_size // 2
    angle = jnp.where(by_row, grid_row, at_row - GRID_W * grid_row) * freq_ref[...]
    cos_ref[...] = jnp.cos(angle)
    sin_ref[...] = jnp.sin(angle)
    kv_all[own_rows, :kv_width] = turned_heads(head_size, raw_k, kg_ref, cos_ref, sin_ref)
    kv_all[own_rows, kv_width:] = raw_v[...]
    for k in range(3):
        weight_move(k, 0, tp, y, "x")
        weight_move(k, 0, tp, y, "core")
    kv_serve(0, None)
    weight_move(GATE, 0, tp, y, "y")
    for p in range(1, n):
        weight_line(GATE, p)
    turned = turned_heads(head_size, raw_q, qg_ref, cos_ref, sin_ref).astype(jnp.float32)
    turned = turned * head_size ** (-0.5)
    group = q_rows // (2 * tok)
    for at in range(raw_q.shape[1] // lanes):
        together = turned[:, at * lanes:(at + 1) * lanes]
        swapped = pltpu.roll(together, head_size, 1)
        low = lax.broadcasted_iota(jnp.int32, together.shape, 1) < head_size
        key_head, g = 2 * at // group, 2 * at % group
        pair, side = key_head // 2, key_head % 2
        for extra in range(2):
            source = together if extra == side else swapped
            kept_lanes = jnp.where(low if side == 0 else jnp.logical_not(low), source, 0.0)
            first = (side * group + g + extra) * tok
            q_ref[pair, first:first + tok, :] = kept_lanes.astype(jnp.bfloat16)

    def all_lines(k):
        for p in range(1, n):
            weight_line(k, p)

    serve = [(k, d) for k in range(3) for d in range(1, n)]
    over_both = [(k, d) for k in range(3) for d in range(n)]
    over_x = sorted(over_both, key=lambda what: what[1] > 0)
    over_y = list(over_x)
    queues = {"s": (weight_serve, serve), "x": (cross_x, over_x), "y": (cross_y, over_y), "b": (cross_both, over_both), "l": (all_lines, [(UP,), (DOWN,)])}

    def work(plan):
        for letter in plan:
            task, queue = queues[letter]
            if queue:
                task(*queue.pop(0))

    crossing = [None]
    for at, step in enumerate(arrivals):
        for j in (1, 0):
            for e in step:
                kv_serve(j, e)
            if at == n - 2:
                work("s")
        if at < 2:
            weight_move(at + 1, 0, tp, y, "y")
        work(("", "xys", "l")[max(0, at - n + 4)])
        for j in (1, 0):
            for e in crossing:
                kv_cross(j, e)
        if at == n - 3:
            work("xy")
        crossing = step
    for j in (1, 0):
        for e in crossing:
            kv_cross(j, e)
    work("xy")
    kv_finish()
    plans = ["xy", "xy", "xy", "", "", "l"]
    for at in range(pairs * per_pair):
        attend(at)
        work(plans[at % len(plans)])
    assemble()
    own_wo.wait()
    project()
    send(("proj",), None, lambda: proj_out, lambda: proj_in, partner)
    project_own()
    work("ss")
    land(("proj",), None, lambda: proj_in)
    normalize()
    for f in range(2):
        rows_serve(f, None)

    def rows_step(at):
        for f in range(2):
            for e in arrivals[at]:
                rows_serve(f, e)

    work("xysxy")
    rows_step(0)
    work("ssxy")
    while over_both[0][0] < UP:
        work("b")
    rows_step(1)
    work("s")
    while over_both[0][0] < DOWN:
        work("b")
    own_each(lambda copy: copy.wait())
    weight_finish(GATE)
    weight_finish(UP)
    upper_half = lax.div(z, n // 2)
    feed(upper_half)
    work("xy")
    for at in range(2, n - 1):
        rows_step(at)
    work("xy")
    feed(1 - upper_half)
    work("xy" * len(over_x))
    weight_finish(DOWN)
    for g in (0, 1):
        lower(g)
        sum_step(g, n - 1)
    for g in (0, 1):
        sum_step(g, n - 2)
    work("b" * len(over_both))
    weight_finish(DOWN, True)
    for g in (2, 3):
        lower(g)
        sum_step(g, n - 1)
    for two in ((0, 1), (2, 3)):
        for d in range(n - 2, 0, -1):
            for g in two:
                if d < n - 2 or g > 1:
                    sum_step(g, d)
    for g in range(groups):
        sum_finish(g)
    for g in range(groups):
        for at in range(n // 2):
            out_copy(g, at).wait()
    for condition, make in sent:
        when(condition, lambda: make().wait_send())
    assert len(slots) + 3 * n == recv_sem.shape[0]


def fast_body(n, queries, keys, values, q_gain, k_gain, w_out, residual, norm_gain, w_gate, w_up, w_down):
    tok_rows = queries.shape[0]
    head_size = q_gain.shape[0]
    q_heads = queries.shape[1] // head_size
    kv_heads = keys.shape[1] // head_size
    q_group = q_heads // kv_heads
    if 2 * w_gate.shape[1] % (n * BLOCK) or n % 2:
        return body(
            queries, keys, values, q_gain, k_gain, w_out, residual, norm_gain, w_gate, w_up, w_down
        )
    n_sp = 4 * n
    half_size = head_size // 2
    inv_freq = np.float32(THETA) ** (-np.arange(0, half_size, 2, dtype=np.float32) / half_size)
    frequencies = jnp.asarray(np.tile(inv_freq, 8)[None, :], jnp.float32)
    pairs = kv_heads // 2
    padded = (pairs, 2 * q_group * tok_rows, 2 * head_size)
    kv_width = keys.shape[1] + values.shape[1]
    tokens = n_sp * tok_rows
    any_space = pl.BlockSpec(memory_space=pl.ANY)
    vmem = pl.BlockSpec(memory_space=pltpu.VMEM)
    own_count, width = residual.shape
    depth_in, units = w_gate.shape
    lanes_down = w_down.shape[1]
    slab = 2 * units // n
    group_rows = n * own_count
    bf16, f32 = jnp.bfloat16, jnp.float32
    return pl.pallas_call(
        functools.partial(layer_kernel, n, head_size),
        out_shape=jax.ShapeDtypeStruct(residual.shape, bf16),
        in_specs=[vmem] * 8 + [any_space] * 4,
        out_specs=any_space,
        scratch_shapes=[
            pltpu.VMEM(padded, bf16),
            pltpu.VMEM((tokens, kv_width), bf16),
            pltpu.VMEM((n_sp * depth_in, slab), bf16),
            pltpu.VMEM((n_sp * depth_in, slab), bf16),
            pltpu.VMEM((slab, n_sp * lanes_down), bf16),
            pltpu.VMEM(w_out.shape, bf16),
            pltpu.VMEM(padded, bf16),
            pltpu.VMEM(queries.shape, bf16),
            pltpu.VMEM((own_count, width), bf16),
            pltpu.VMEM((own_count, width), bf16),
            pltpu.VMEM((own_count, width), f32),
            pltpu.VMEM((group_rows, width), bf16),
            pltpu.VMEM((group_rows, slab), bf16),
            pltpu.VMEM((group_rows, width), f32),
            pltpu.VMEM((group_rows, width), bf16),
            pltpu.VMEM((4, 2, n - 1, own_count, width // 4), bf16),
            pltpu.VMEM((own_count, width), bf16),
            pltpu.VMEM((tok_rows, 2 * head_size), f32),
            pltpu.VMEM((tok_rows, 2 * head_size), f32),
            pltpu.SemaphoreType.DMA((4,)),
            pltpu.SemaphoreType.DMA((2 * n,)),
            pltpu.SemaphoreType.DMA((1,)),
            pltpu.SemaphoreType.DMA((message_count(n),)),
        ],
        compiler_params=pltpu.CompilerParams(
            collective_id=0, has_side_effects=True, vmem_limit_bytes=63 * 1024 * 1024
        ),
        name="layer",
    )(
        queries, keys, values, q_gain[None, :], k_gain[None, :], frequencies,
        residual, norm_gain[None, :], w_out, w_gate, w_up, w_down)


def solution(mesh):
    n = line_of_chips(mesh)
    inner = body if n is None else functools.partial(fast_body, n)
    return jax.shard_map(
        inner,
        mesh=mesh,
        in_specs=(
            P("sp", "tp"),
            P("sp", "tp"),
            P("sp", "tp"),
            P(),
            P(),
            P("tp", None),
            P(("sp", "tp"), None),
            P(),
            P("sp", "tp"),
            P("sp", "tp"),
            P("tp", "sp"),
        ),
        out_specs=P(("sp", "tp"), None),
        check_vma=False,
    )
```

```python
import functools
import math

import jax
import jax.numpy as jnp
import numpy as np
from jax import lax
from jax.experimental import pallas as pl
from jax.experimental.pallas import tpu as pltpu
from jax.sharding import PartitionSpec as P

GRID_W = 128


EPS = 1e-06
THETA = 10000.0


def turn_half(part, angle):
    quarter = part.shape[-1] // 2
    cos_table = jnp.cos(angle)[:, None, :]
    sin_table = jnp.sin(angle)[:, None, :]
    first_part = part[..., :quarter]
    second_part = part[..., quarter:]
    return jnp.concatenate(
        [
            first_part * cos_table - second_part * sin_table,
            first_part * sin_table + second_part * cos_table,
        ],
        axis=-1,
    )


def head_norm_rope(flat, gain, offset, head_count):
    tok_rows = flat.shape[0]
    head_size = flat.shape[1] // head_count
    heads = flat.astype(jnp.float32).reshape(tok_rows, head_count, head_size)
    heads = heads * lax.rsqrt(jnp.mean(heads * heads, axis=-1, keepdims=True) + EPS) * gain
    positions = offset + jnp.arange(tok_rows, dtype=jnp.int32)
    row_pos = (positions // GRID_W).astype(jnp.float32)
    col_pos = (positions % GRID_W).astype(jnp.float32)
    half_size = head_size // 2
    inv_freq = THETA ** (-jnp.arange(0, half_size, 2, dtype=jnp.float32) / half_size)
    turned = jnp.concatenate(
        [
            turn_half(heads[..., :half_size], row_pos[:, None] * inv_freq[None, :]),
            turn_half(heads[..., half_size:], col_pos[:, None] * inv_freq[None, :]),
        ],
        axis=-1,
    )
    return turned.reshape(tok_rows, head_count * head_size).astype(jnp.bfloat16)


def body(queries, keys, values, q_gain, k_gain, w_out, residual, norm_gain, w_gate, w_up, w_down):
    tok_rows = queries.shape[0]
    head_size = q_gain.shape[0]
    q_heads = queries.shape[1] // head_size
    kv_heads = keys.shape[1] // head_size
    q_group = q_heads // kv_heads
    offset = lax.axis_index("sp") * tok_rows
    q_rot = head_norm_rope(queries, q_gain, offset, q_heads)
    k_rot = head_norm_rope(keys, k_gain, offset, kv_heads)
    query_groups = q_rot.reshape(tok_rows, kv_heads, q_group, head_size)
    score_scale = head_size ** (-0.5)
    start_state = (
        jnp.full((kv_heads, q_group, tok_rows), -1e30, jnp.float32),
        jnp.zeros((kv_heads, q_group, tok_rows), jnp.float32),
        jnp.zeros((kv_heads, q_group, tok_rows, head_size), jnp.float32),
    )
    running = start_state
    key_piece = lax.all_gather(k_rot, "sp", axis=0, tiled=True)
    value_piece = lax.all_gather(values, "sp", axis=0, tiled=True)
    piece_len = key_piece.shape[0]
    block_len = math.gcd(piece_len, 512)
    blocks = piece_len // block_len
    key_blocks = key_piece.reshape(blocks, block_len, kv_heads, head_size)
    value_blocks = value_piece.reshape(blocks, block_len, kv_heads, head_size)

    def update(state, block_pair):
        prior_max, totals, accum = state
        key_block, value_block = block_pair
        scores = (
            jnp.einsum(
                "qhgd,khd->hgqk", query_groups, key_block, preferred_element_type=jnp.float32
            )
            * score_scale
        )
        new_max = jnp.maximum(prior_max, jnp.max(scores, axis=-1))
        weights = jnp.exp(scores - new_max[..., None])
        factor = jnp.exp(prior_max - new_max)
        totals = totals * factor + jnp.sum(weights, axis=-1)
        accum = accum * factor[..., None] + jnp.einsum(
            "hgqk,khd->hgqd",
            weights.astype(jnp.bfloat16),
            value_block,
            preferred_element_type=jnp.float32,
        )
        return ((new_max, totals, accum), None)

    running, unused = lax.scan(update, running, (key_blocks, value_blocks))
    final_max, totals, accum = running
    mixed = accum / totals[..., None]
    attn = (
        jnp.transpose(mixed, (2, 0, 1, 3))
        .reshape(tok_rows, q_heads * head_size)
        .astype(jnp.bfloat16)
    )
    own_rows = lax.all_to_all(attn, "tp", split_axis=0, concat_axis=1, tiled=True)
    columns = own_rows
    proj = jnp.dot(
        columns, lax.all_gather(w_out, "tp", axis=0, tiled=True), preferred_element_type=jnp.float32
    )
    mid = residual.astype(jnp.float32) + proj
    normed = (
        mid * lax.rsqrt(jnp.mean(mid * mid, axis=-1, keepdims=True) + EPS) * norm_gain
    ).astype(jnp.bfloat16)
    gathered = lax.all_gather(normed, "tp", axis=0, tiled=True)
    columns = gathered
    gate = jnp.dot(
        columns,
        lax.all_gather(w_gate, "sp", axis=0, tiled=True),
        preferred_element_type=jnp.float32,
    )
    up_part = jnp.dot(
        columns, lax.all_gather(w_up, "sp", axis=0, tiled=True), preferred_element_type=jnp.float32
    )
    hidden = (jax.nn.silu(gate) * up_part).astype(jnp.bfloat16)
    terms = jnp.dot(
        hidden, lax.all_gather(w_down, "sp", axis=1, tiled=True), preferred_element_type=jnp.float32
    )
    down = lax.psum_scatter(
        terms.astype(jnp.bfloat16), "tp", scatter_dimension=0, tiled=True
    ).astype(jnp.float32)
    return (mid + 0.5 * down).astype(jnp.bfloat16)


MESH = pl.DeviceIdType.MESH
BLOCK = 128


def line_of_chips(mesh):
    count = mesh.shape["sp"]
    try:
        places = [(tuple(d.coords), d.core_on_chip) for d in mesh.devices[:, 0].flat]
    except AttributeError:
        return None
    if count % 4 or count < 12 or mesh.shape["tp"] != 2:
        return None
    first = places[0][0]
    for at, (coords, core) in enumerate(places):
        chip = at // 2
        want = (first[0], first[1] + chip % 2, first[2] + chip // 2)
        if coords != want or core != at % 2:
            return None
    return count // 4


def message_count(n):
    events = 2 * (n - 1)
    keys_and_values = 2 * events + 2 * (events + 1) + 1
    weights = 3 * n + 9 * n + 4
    return keys_and_values + weights + 1 + 2 * events + 8 * (n - 1)


def turned_heads(head_size, x_ref, g_ref, cos_ref, sin_ref):
    x = x_ref[...].astype(jnp.float32)
    width = x.shape[1]
    lane = lax.broadcasted_iota(jnp.int32, (width, width), 0) // head_size
    other = lax.broadcasted_iota(jnp.int32, (width, width), 1) // head_size
    same = (lane == other).astype(jnp.float32)
    mean = jnp.dot(
        x * x, same, preferred_element_type=jnp.float32, precision=lax.Precision.HIGHEST
    ) * (1.0 / head_size)
    h = x * lax.rsqrt(mean + EPS) * jnp.concatenate([g_ref[...]] * (width // head_size), axis=1)
    quarter = head_size // 4
    repeats = width // cos_ref.shape[1]
    cos_table = jnp.concatenate([cos_ref[...]] * repeats, axis=1)
    sin_table = jnp.concatenate([sin_ref[...]] * repeats, axis=1)
    at = lax.broadcasted_iota(jnp.int32, x.shape, 1)
    is_first = (at // quarter) % 2 == 0
    ahead = pltpu.roll(h, width - quarter, 1)
    behind = pltpu.roll(h, quarter, 1)
    turned = h * cos_table + jnp.where(is_first, -ahead, behind) * sin_table
    return turned.astype(jnp.bfloat16)


def when(condition, action):
    if condition is None:
        action()
    else:
        pl.when(condition)(action)


def both(one, other):
    if one is None:
        return other
    if other is None:
        return one
    return jnp.logical_and(one, other)


def layer_kernel(
    n, head_size,
    raw_q, raw_k, raw_v, qg_ref, kg_ref, freq_ref, res_ref, gain_ref, wo_in, wg_in, wu_in, wd_in,
    out_ref,
    q_ref, kv_all, wg_all, wu_all, wd_all, wo_own, attn, context, proj_out, proj_in, mid, normed, hidden,
    part, leaving, line_in, out_own, cos_ref, sin_ref, own_sem, out_sem, send_sem, recv_sem,
):
    sp = lax.axis_index("sp")
    tp = lax.axis_index("tp")
    core = lax.rem(sp, 2)
    y = lax.rem(lax.div(sp, 2), 2)
    z = lax.div(sp, 4)

    def device(zz, yy, cc):
        return (zz * 2 + yy) * 2 + cc

    def wrapped(zz):
        return lax.rem(zz + n, n)

    sibling = (device(z, y, 1 - core), tp)
    across = (device(z, 1 - y, core), tp)
    partner = (sp, 1 - tp)

    def level(zz):
        return (device(zz, y, core), tp)

    barrier = pltpu.get_barrier_semaphore()
    greeted = [sibling, across, partner] + [level(wrapped(z + d)) for d in range(1, n)]
    for target in greeted:
        pl.semaphore_signal(barrier, inc=1, device_id=target, device_id_type=MESH)
    pl.semaphore_wait(barrier, len(greeted))

    slots = {}
    sent = []

    def message(key, src, dst, target):
        slot = key
        if isinstance(key, tuple):
            slot = slots.setdefault(key, 3 * n + len(slots))
        return pltpu.make_async_remote_copy(
            src_ref=src, dst_ref=dst, send_sem=send_sem.at[0], recv_sem=recv_sem.at[slot],
            device_id=target, device_id_type=MESH,
        )

    def send(key, condition, src, dst, target):
        def make():
            return message(key, src(), dst(), target)

        when(condition, lambda: make().start())
        sent.append((condition, make))

    def land(key, condition, piece):
        when(condition, lambda: message(key, piece(), piece(), partner).wait_recv())

    near = [z]
    for p in range(1, n):
        level_at = 0
        for zz in range(n):
            order = sorted(range(n), key=lambda other: (abs(other - zz), -abs(2 * other - n + 1)))
            level_at = jnp.where(z == zz, order[p], level_at)
        near.append(level_at)

    arrivals = [[(s, w) for w in range(2)] for s in range(n - 1)]
    events = [None] + [e for step in arrivals for e in step]
    room = (z <= n - 2, z >= 1)
    ahead = (level(z + 1), level(z - 1))

    def home(e):
        if e is None:
            return z
        return z - 1 - e[0] if e[1] == 0 else z + 1 + e[0]

    def real(e):
        if e is None:
            return None
        return z >= e[0] + 1 if e[1] == 0 else z <= n - 2 - e[0]

    def pass_on(name, e, src, dst):
        for w in range(2) if e is None else (e[1],):
            step = 0 if e is None else e[0] + 1
            if step <= n - 2:
                send((name, step, w), both(real(e), room[w]), src, dst, ahead[w])

    tok = raw_q.shape[0]
    kv_width = raw_k.shape[1]

    def kv_piece(j, zz, yy, cc):
        start = pl.multiple_of(device(zz, yy, cc) * tok, tok)
        return kv_all.at[pl.ds(start, tok), j * kv_width:(j + 1) * kv_width]

    def kv_serve(j, e):
        def dst():
            return kv_piece(j, home(e), y, core)

        if e is not None:
            land((("kv", j), e[0], e[1]), real(e), dst)
        src = (lambda: raw_v) if e is None and j == 1 else dst
        pass_on(("kv", j), e, src, dst)
        send(("kv y", j, e), real(e), src, dst, across)
        send(("kv core",), real(e), src, dst, sibling)

    def kv_cross(j, e):
        def piece():
            return kv_piece(j, home(e), 1 - y, core)

        land(("kv y", j, e), real(e), piece)
        send(("kv core",), real(e), piece, piece, sibling)

    def kv_finish():
        land(("kv core",), None, lambda: kv_all.at[:kv_all.shape[0] // 2, :])

    GATE, UP, DOWN = range(3)
    weights_in = (wg_in, wu_in, wd_in)
    rows, units = wg_in.shape
    lanes_down = wd_in.shape[1]
    slab = wg_all.shape[1]
    share = slab // BLOCK

    def first_block(zz, xx):
        return lax.div(zz * share + xx, 2)

    def unit_forms(zz, xx):
        if share % 2 == 0:
            return [(None, share // 2)]
        many = lax.rem(zz + xx, 2) == 1
        return [(jnp.logical_not(many), share // 2), (many, share // 2 + 1)]

    def weight_in(k, zz, count):
        span = pl.ds(pl.multiple_of(first_block(zz, tp) * BLOCK, BLOCK), count * BLOCK)
        return wd_in.at[span, :] if k == DOWN else weights_in[k].at[:, span]

    def weight(k, xx, zz, yy, cc, keeper, count):
        o = device(zz, yy, cc)
        before = xx * (first_block(keeper + 1, 0) - first_block(keeper, 0))
        units_of = pl.ds(pl.multiple_of(before * BLOCK, BLOCK), count * BLOCK)
        if k == DOWN:
            return wd_all.at[units_of, pl.ds(pl.multiple_of(o * lanes_down, lanes_down), lanes_down)]
        return (wg_all, wu_all)[k].at[pl.ds(pl.multiple_of(o * rows, rows), rows), units_of]

    def weight_line(k, p):
        zt = near[p]
        for condition, count in unit_forms(zt, tp):
            send(
                k * n + wrapped(zt - z), condition,
                functools.partial(weight_in, k, zt, count),
                functools.partial(weight, k, tp, z, y, core, zt, count), level(zt),
            )

    def by_x(k, p):
        return (p % 4 < 2, p % 2 == 0, p % 4 < 2)[k]

    def weight_move(k, p, xx, yy, way):
        target = {"x": partner, "y": across, "core": sibling}[way]
        corner = (xx is not tp, yy is not y)
        for condition, count in unit_forms(z, xx):
            dst = functools.partial(weight, k, xx, near[p], yy, core, z, count)
            src = dst
            if p == 0 and corner == (False, False):
                src = functools.partial(weight_in, k, z, count)
            key = ("w", way, k, p, corner)
            if way == "core":
                key = ("w", way, k, k == DOWN and corner[1])
            send(key, condition, src, dst, target)

    other_x, other_y = 1 - tp, 1 - y

    def weight_take(key, k, p, xx, yy, cc):
        for condition, count in unit_forms(z, xx):
            land(key, condition, functools.partial(weight, k, xx, near[p], yy, cc, z, count))

    def weight_land(k, p, way, xx, yy):
        corner = (xx is not tp, yy is not y)
        seen = {"x": (not corner[0], corner[1]), "y": (corner[0], not corner[1])}[way]
        weight_take(("w", way, k, p, seen), k, p, xx, yy, core)

    def weight_arrive(k, p):
        weight_take(k * n + wrapped(z - near[p]), k, p, tp, y, core)

    def weight_serve(k, p):
        if p > 0:
            weight_arrive(k, p)
        weight_move(k, p, tp, y, "y")
        weight_move(k, p, tp, y, "x")
        weight_move(k, p, tp, y, "core")

    def cross_y(k, p):
        weight_land(k, p, "y", tp, other_y)
        if by_x(k, p):
            weight_move(k, p, tp, other_y, "x")
        weight_move(k, p, tp, other_y, "core")

    def cross_x(k, p):
        weight_land(k, p, "x", other_x, y)
        if not by_x(k, p):
            weight_move(k, p, other_x, y, "y")
        weight_move(k, p, other_x, y, "core")

    def cross_both(k, p):
        weight_land(k, p, "x" if by_x(k, p) else "y", other_x, other_y)
        weight_move(k, p, other_x, other_y, "core")

    def own_copy(k, count):
        return pltpu.make_async_copy(
            weight_in(k, z, count), weight(k, tp, z, y, core, z, count), own_sem.at[k]
        )

    def own_each(act):
        for k in range(3):
            for condition, count in unit_forms(z, tp):
                when(condition, lambda: act(own_copy(k, count)))

    own_wo = pltpu.make_async_copy(wo_in, wo_own, own_sem.at[3])

    def weight_finish(k, second=False):
        def bulk():
            if k == DOWN:
                return wd_all.at[:, :wd_all.shape[1] // 4]
            ref = (wg_all, wu_all)[k]
            return ref.at[:ref.shape[0] // 2, :]

        land(("w", "core", k, second), None, bulk)

    pairs, q_rows, lanes = q_ref.shape
    block = math.gcd(q_rows, 256)
    per_pair = q_rows // block

    def attend(at):
        pair, which = at // per_pair, at % per_pair
        span = slice(which * block, (which + 1) * block)
        q = q_ref[pair, span, :]
        k = kv_all[:, pair * lanes:(pair + 1) * lanes]
        v = kv_all[:, (pairs + pair) * lanes:(pairs + pair + 1) * lanes]
        scores = lax.dot_general(
            q, k, (((1,), (1,)), ((), ())), preferred_element_type=jnp.float32
        )
        weights = jnp.exp(scores - jnp.max(scores, axis=-1, keepdims=True))
        total = jnp.sum(weights, axis=-1, keepdims=True)
        mixed = jnp.dot(weights.astype(jnp.bfloat16), v, preferred_element_type=jnp.float32)
        attn[pair, span, :] = (mixed / total).astype(jnp.bfloat16)

    def assemble():
        group = q_rows // (2 * tok)
        pieces = []
        for pair in range(pairs):
            for side in range(2):
                for g in range(0, group, 2):
                    lower = attn[pair, pl.ds((side * group + g) * tok, tok), :].astype(jnp.float32)
                    upper = attn[pair, pl.ds((side * group + g + 1) * tok, tok), :].astype(jnp.float32)
                    if side == 1:
                        lower = pltpu.roll(lower, head_size, 1)
                    else:
                        upper = pltpu.roll(upper, head_size, 1)
                    lane = lax.broadcasted_iota(jnp.int32, lower.shape, 1)
                    pieces.append(jnp.where(lane < head_size, lower, upper).astype(jnp.bfloat16))
        context[...] = jnp.concatenate(pieces, axis=1)

    own_count, width = res_ref.shape
    rows_of = own_count // 2
    mine = pl.ds(pl.multiple_of(tp * own_count, own_count), own_count)
    theirs = pl.ds(pl.multiple_of((1 - tp) * own_count, own_count), own_count)

    def whole(zz):
        return pl.ds(pl.multiple_of(zz * own_count, own_count), own_count)

    def rows_at(zz, f):
        return pl.ds(pl.multiple_of((zz * 2 + f) * rows_of, rows_of), rows_of)

    wide = math.gcd(width, 512)

    def project():
        given = context[theirs, :]
        for at in range(0, width, wide):
            cols = slice(at, at + wide)
            proj_out[:, cols] = jnp.dot(
                given, wo_own[:, cols], preferred_element_type=jnp.float32
            ).astype(jnp.bfloat16)

    def project_own():
        held = context[mine, :]
        for at in range(0, width, wide):
            cols = slice(at, at + wide)
            mid[:, cols] = res_ref[:, cols].astype(jnp.float32) + jnp.dot(
                held, wo_own[:, cols], preferred_element_type=jnp.float32
            )

    def normalize():
        value = mid[...] + proj_in[...].astype(jnp.float32)
        mid[...] = value
        scale = lax.rsqrt(jnp.mean(value * value, axis=-1, keepdims=True) + EPS)
        normed[whole(z), :] = (value * scale * gain_ref[...]).astype(jnp.bfloat16)

    def rows_serve(f, e):
        def piece():
            return normed.at[rows_at(home(e), f), :]

        if e is not None:
            land((("rows", f), e[0], e[1]), real(e), piece)
        pass_on(("rows", f), e, piece, piece)

    tile = 2 * lanes_down

    def feed():
        def some(cols):
            x = normed[...]
            gate = jnp.dot(x, wg_all[:, cols], preferred_element_type=jnp.float32)
            up = jnp.dot(x, wu_all[:, cols], preferred_element_type=jnp.float32)
            hidden[:, cols] = (gate / (1.0 + jnp.exp(-gate)) * up).astype(jnp.bfloat16)

        @pl.loop(0, slab // tile)
        def _(at):
            some(pl.ds(pl.multiple_of(at * tile, tile), tile))

        if slab % tile:
            some(slice(slab - slab % tile, slab))

    groups = 4
    cols_of = width // groups

    def result_columns(g, at):
        zs = g % 2 * (n // 2) + at
        start = (zs * 4 + 2 * (y, other_y)[g // 2]) * lanes_down
        return pl.ds(pl.multiple_of(start, tile), tile)

    def lower(g):
        @pl.loop(0, n // 2)
        def _(at):
            cols = pl.ds(pl.multiple_of(g * cols_of + at * tile, tile), tile)
            part[:, cols] = jnp.dot(
                hidden[...], wd_all[:, result_columns(g, at)], preferred_element_type=jnp.float32
            )

    def columns(g):
        return slice(g * cols_of, (g + 1) * cols_of)

    def add(zz, f, ref):
        part[whole(zz), columns(f)] = part[whole(zz), columns(f)] + ref[...].astype(jnp.float32)

    def sum_step(f, d, ends=None):
        for w in range(2):
            inside = z <= n - 1 - d if w == 0 else z >= d
            if ends is not None:
                inside = both(inside, jnp.logical_not(room[1 - w]) if ends else room[1 - w])
            sum_send(f, w, d, inside)

    def sum_send(f, w, d, inside):
        zz = z + d if w == 0 else z - d
        if d < n - 1:
            def take():
                message(("sum", f, w, d + 1), line_in.at[f, w, d], line_in.at[f, w, d], partner).wait_recv()
                add(zz, f, line_in.at[f, w, d])

            when(both(inside, room[1 - w]), take)

        def put():
            leaving[whole(zz), columns(f)] = part[whole(zz), columns(f)].astype(jnp.bfloat16)

        when(inside, put)
        send(
            ("sum", f, w, d), inside,
            lambda: leaving.at[whole(zz), columns(f)], lambda: line_in.at[f, w, d - 1], ahead[w],
        )

    def out_copy(g, at):
        cols = result_columns(g, at)
        return pltpu.make_async_copy(
            out_own.at[:, cols], out_ref.at[:, cols], out_sem.at[g * (n // 2) + at]
        )

    def sum_finish(f):
        for w in range(2):
            def take():
                message(("sum", f, w, 1), line_in.at[f, w, 0], line_in.at[f, w, 0], partner).wait_recv()
                add(z, f, line_in.at[f, w, 0])

            when(room[1 - w], take)
        for at in range(n // 2):
            cols = result_columns(f, at)
            start = f * cols_of + at * tile
            down = part[whole(z), start:start + tile]
            out_own[:, cols] = (mid[:, cols] + 0.5 * down).astype(jnp.bfloat16)
            out_copy(f, at).start()

    own_each(lambda copy: copy.start())
    own_wo.start()
    kv_serve(1, None)
    own_rows = pl.ds(pl.multiple_of(sp * tok, tok), tok)
    at_row = (sp * tok + lax.broadcasted_iota(jnp.int32, cos_ref.shape, 0)).astype(jnp.float32)
    grid_row = jnp.floor(at_row * (1.0 / GRID_W))
    lane = lax.broadcasted_iota(jnp.int32, cos_ref.shape, 1)
    by_row = jnp.bitwise_and(lane, head_size - 1) < head_size // 2
    angle = jnp.where(by_row, grid_row, at_row - GRID_W * grid_row) * freq_ref[...]
    cos_ref[...] = jnp.cos(angle)
    sin_ref[...] = jnp.sin(angle)
    kv_all[own_rows, :kv_width] = turned_heads(head_size, raw_k, kg_ref, cos_ref, sin_ref)
    kv_all[own_rows, kv_width:] = raw_v[...]
    for k in range(3):
        weight_move(k, 0, tp, y, "x")
        weight_move(k, 0, tp, y, "core")
    kv_serve(0, None)
    weight_move(GATE, 0, tp, y, "y")
    for p in range(1, n):
        weight_line(GATE, p)
    turned = turned_heads(head_size, raw_q, qg_ref, cos_ref, sin_ref).astype(jnp.float32)
    turned = turned * head_size ** (-0.5)
    group = q_rows // (2 * tok)
    for at in range(raw_q.shape[1] // lanes):
        together = turned[:, at * lanes:(at + 1) * lanes]
        swapped = pltpu.roll(together, head_size, 1)
        low = lax.broadcasted_iota(jnp.int32, together.shape, 1) < head_size
        key_head, g = 2 * at // group, 2 * at % group
        pair, side = key_head // 2, key_head % 2
        for extra in range(2):
            source = together if extra == side else swapped
            kept_lanes = jnp.where(low if side == 0 else jnp.logical_not(low), source, 0.0)
            first = (side * group + g + extra) * tok
            q_ref[pair, first:first + tok, :] = kept_lanes.astype(jnp.bfloat16)

    def all_lines(k):
        for p in range(1, n):
            weight_line(k, p)

    serve = [(k, d) for k in range(3) for d in range(1, n)]
    over_both = [(k, d) for k in range(3) for d in range(n)]
    over_x = sorted(over_both, key=lambda what: what[1] > 0)
    over_y = list(over_x)
    queues = {"s": (weight_serve, serve), "x": (cross_x, over_x), "y": (cross_y, over_y), "b": (cross_both, over_both), "l": (all_lines, [(UP,), (DOWN,)])}

    def work(plan):
        for letter in plan:
            task, queue = queues[letter]
            if queue:
                task(*queue.pop(0))

    crossing = [None]
    for at, step in enumerate(arrivals):
        for j in (1, 0):
            for e in step:
                kv_serve(j, e)
        if at == 0:
            weight_move(UP, 0, tp, y, "y")
        work(("", "xys", "ssl")[max(0, at - n + 4)])
        for j in (1, 0):
            for e in crossing:
                kv_cross(j, e)
        if at == n - 3:
            work("xy")
        crossing = step
    for j in (1, 0):
        for e in crossing:
            kv_cross(j, e)
    weight_move(DOWN, 0, tp, y, "y")
    kv_finish()
    plans = ["", "", "", "", "", "l"]
    for at in range(pairs * per_pair):
        attend(at)
        work(plans[at % len(plans)])
    assemble()
    own_wo.wait()
    project()
    send(("proj",), None, lambda: proj_out, lambda: proj_in, partner)
    project_own()
    work("xyxyxysxys")
    land(("proj",), None, lambda: proj_in)
    normalize()
    for f in range(2):
        rows_serve(f, None)

    def rows_step(at):
        for f in range(2):
            for e in arrivals[at]:
                rows_serve(f, e)

    work("xysxy")
    rows_step(0)
    work("xyss")
    while over_both[0][0] < UP:
        work("b")
    rows_step(1)
    work("s")
    while over_both[0][0] < DOWN:
        work("b")
    own_each(lambda copy: copy.wait())
    weight_finish(GATE)
    weight_finish(UP)
    for at in range(2, n - 1):
        rows_step(at)
    work("xy")
    feed()
    work("xy" * len(over_x))
    weight_finish(DOWN)
    for g in (0, 1):
        lower(g)
        sum_step(g, n - 1)
    for g in (0, 1):
        sum_step(g, n - 2)
    work("b" * len(over_both))
    weight_finish(DOWN, True)
    for g in (2, 3):
        lower(g)
        sum_step(g, n - 1)
    for two in ((0, 1), (2, 3)):
        for d in range(n - 2, 0, -1):
            for g in two:
                if d < n - 2 or g > 1:
                    sum_step(g, d, False if d == 1 else None)
    for g in range(groups):
        sum_step(g, 1, True)
    for g in range(groups):
        sum_finish(g)
    for g in range(groups):
        for at in range(n // 2):
            out_copy(g, at).wait()
    for condition, make in sent:
        when(condition, lambda: make().wait_send())
    assert len(slots) + 3 * n == recv_sem.shape[0]


def fast_body(n, queries, keys, values, q_gain, k_gain, w_out, residual, norm_gain, w_gate, w_up, w_down):
    tok_rows = queries.shape[0]
    head_size = q_gain.shape[0]
    q_heads = queries.shape[1] // head_size
    kv_heads = keys.shape[1] // head_size
    q_group = q_heads // kv_heads
    if 2 * w_gate.shape[1] % (n * BLOCK) or n % 2:
        return body(
            queries, keys, values, q_gain, k_gain, w_out, residual, norm_gain, w_gate, w_up, w_down
        )
    n_sp = 4 * n
    half_size = head_size // 2
    inv_freq = np.float32(THETA) ** (-np.arange(0, half_size, 2, dtype=np.float32) / half_size)
    frequencies = jnp.asarray(np.tile(inv_freq, 8)[None, :], jnp.float32)
    pairs = kv_heads // 2
    padded = (pairs, 2 * q_group * tok_rows, 2 * head_size)
    kv_width = keys.shape[1] + values.shape[1]
    tokens = n_sp * tok_rows
    any_space = pl.BlockSpec(memory_space=pl.ANY)
    vmem = pl.BlockSpec(memory_space=pltpu.VMEM)
    own_count, width = residual.shape
    depth_in, units = w_gate.shape
    lanes_down = w_down.shape[1]
    slab = 2 * units // n
    group_rows = n * own_count
    bf16, f32 = jnp.bfloat16, jnp.float32
    return pl.pallas_call(
        functools.partial(layer_kernel, n, head_size),
        out_shape=jax.ShapeDtypeStruct(residual.shape, bf16),
        in_specs=[vmem] * 8 + [any_space] * 4,
        out_specs=any_space,
        scratch_shapes=[
            pltpu.VMEM(padded, bf16),
            pltpu.VMEM((tokens, kv_width), bf16),
            pltpu.VMEM((n_sp * depth_in, slab), bf16),
            pltpu.VMEM((n_sp * depth_in, slab), bf16),
            pltpu.VMEM((slab, n_sp * lanes_down), bf16),
            pltpu.VMEM(w_out.shape, bf16),
            pltpu.VMEM(padded, bf16),
            pltpu.VMEM(queries.shape, bf16),
            pltpu.VMEM((own_count, width), bf16),
            pltpu.VMEM((own_count, width), bf16),
            pltpu.VMEM((own_count, width), f32),
            pltpu.VMEM((group_rows, width), bf16),
            pltpu.VMEM((group_rows, slab), bf16),
            pltpu.VMEM((group_rows, width), f32),
            pltpu.VMEM((group_rows, width), bf16),
            pltpu.VMEM((4, 2, n - 1, own_count, width // 4), bf16),
            pltpu.VMEM((own_count, width), bf16),
            pltpu.VMEM((tok_rows, 2 * head_size), f32),
            pltpu.VMEM((tok_rows, 2 * head_size), f32),
            pltpu.SemaphoreType.DMA((4,)),
            pltpu.SemaphoreType.DMA((2 * n,)),
            pltpu.SemaphoreType.DMA((1,)),
            pltpu.SemaphoreType.DMA((message_count(n),)),
        ],
        compiler_params=pltpu.CompilerParams(
            collective_id=0, has_side_effects=True, vmem_limit_bytes=63 * 1024 * 1024
        ),
        name="layer",
    )(
        queries, keys, values, q_gain[None, :], k_gain[None, :], frequencies,
        residual, norm_gain[None, :], w_out, w_gate, w_up, w_down)


def solution(mesh):
    n = line_of_chips(mesh)
    inner = body if n is None else functools.partial(fast_body, n)
    return jax.shard_map(
        inner,
        mesh=mesh,
        in_specs=(
            P("sp", "tp"),
            P("sp", "tp"),
            P("sp", "tp"),
            P(),
            P(),
            P("tp", None),
            P(("sp", "tp"), None),
            P(),
            P("sp", "tp"),
            P("sp", "tp"),
            P("tp", "sp"),
        ),
        out_specs=P(("sp", "tp"), None),
        check_vma=False,
    )
```

```python
import functools
import math

import jax
import jax.numpy as jnp
import numpy as np
from jax import lax
from jax.experimental import pallas as pl
from jax.experimental.pallas import tpu as pltpu
from jax.sharding import PartitionSpec as P

GRID_W = 128


EPS = 1e-06
THETA = 10000.0


def turn_half(part, angle):
    quarter = part.shape[-1] // 2
    cos_table = jnp.cos(angle)[:, None, :]
    sin_table = jnp.sin(angle)[:, None, :]
    first_part = part[..., :quarter]
    second_part = part[..., quarter:]
    return jnp.concatenate(
        [
            first_part * cos_table - second_part * sin_table,
            first_part * sin_table + second_part * cos_table,
        ],
        axis=-1,
    )


def head_norm_rope(flat, gain, offset, head_count):
    tok_rows = flat.shape[0]
    head_size = flat.shape[1] // head_count
    heads = flat.astype(jnp.float32).reshape(tok_rows, head_count, head_size)
    heads = heads * lax.rsqrt(jnp.mean(heads * heads, axis=-1, keepdims=True) + EPS) * gain
    positions = offset + jnp.arange(tok_rows, dtype=jnp.int32)
    row_pos = (positions // GRID_W).astype(jnp.float32)
    col_pos = (positions % GRID_W).astype(jnp.float32)
    half_size = head_size // 2
    inv_freq = THETA ** (-jnp.arange(0, half_size, 2, dtype=jnp.float32) / half_size)
    turned = jnp.concatenate(
        [
            turn_half(heads[..., :half_size], row_pos[:, None] * inv_freq[None, :]),
            turn_half(heads[..., half_size:], col_pos[:, None] * inv_freq[None, :]),
        ],
        axis=-1,
    )
    return turned.reshape(tok_rows, head_count * head_size).astype(jnp.bfloat16)


def body(queries, keys, values, q_gain, k_gain, w_out, residual, norm_gain, w_gate, w_up, w_down):
    tok_rows = queries.shape[0]
    head_size = q_gain.shape[0]
    q_heads = queries.shape[1] // head_size
    kv_heads = keys.shape[1] // head_size
    q_group = q_heads // kv_heads
    offset = lax.axis_index("sp") * tok_rows
    q_rot = head_norm_rope(queries, q_gain, offset, q_heads)
    k_rot = head_norm_rope(keys, k_gain, offset, kv_heads)
    query_groups = q_rot.reshape(tok_rows, kv_heads, q_group, head_size)
    score_scale = head_size ** (-0.5)
    start_state = (
        jnp.full((kv_heads, q_group, tok_rows), -1e30, jnp.float32),
        jnp.zeros((kv_heads, q_group, tok_rows), jnp.float32),
        jnp.zeros((kv_heads, q_group, tok_rows, head_size), jnp.float32),
    )
    running = start_state
    key_piece = lax.all_gather(k_rot, "sp", axis=0, tiled=True)
    value_piece = lax.all_gather(values, "sp", axis=0, tiled=True)
    piece_len = key_piece.shape[0]
    block_len = math.gcd(piece_len, 512)
    blocks = piece_len // block_len
    key_blocks = key_piece.reshape(blocks, block_len, kv_heads, head_size)
    value_blocks = value_piece.reshape(blocks, block_len, kv_heads, head_size)

    def update(state, block_pair):
        prior_max, totals, accum = state
        key_block, value_block = block_pair
        scores = (
            jnp.einsum(
                "qhgd,khd->hgqk", query_groups, key_block, preferred_element_type=jnp.float32
            )
            * score_scale
        )
        new_max = jnp.maximum(prior_max, jnp.max(scores, axis=-1))
        weights = jnp.exp(scores - new_max[..., None])
        factor = jnp.exp(prior_max - new_max)
        totals = totals * factor + jnp.sum(weights, axis=-1)
        accum = accum * factor[..., None] + jnp.einsum(
            "hgqk,khd->hgqd",
            weights.astype(jnp.bfloat16),
            value_block,
            preferred_element_type=jnp.float32,
        )
        return ((new_max, totals, accum), None)

    running, unused = lax.scan(update, running, (key_blocks, value_blocks))
    final_max, totals, accum = running
    mixed = accum / totals[..., None]
    attn = (
        jnp.transpose(mixed, (2, 0, 1, 3))
        .reshape(tok_rows, q_heads * head_size)
        .astype(jnp.bfloat16)
    )
    own_rows = lax.all_to_all(attn, "tp", split_axis=0, concat_axis=1, tiled=True)
    columns = own_rows
    proj = jnp.dot(
        columns, lax.all_gather(w_out, "tp", axis=0, tiled=True), preferred_element_type=jnp.float32
    )
    mid = residual.astype(jnp.float32) + proj
    normed = (
        mid * lax.rsqrt(jnp.mean(mid * mid, axis=-1, keepdims=True) + EPS) * norm_gain
    ).astype(jnp.bfloat16)
    gathered = lax.all_gather(normed, "tp", axis=0, tiled=True)
    columns = gathered
    gate = jnp.dot(
        columns,
        lax.all_gather(w_gate, "sp", axis=0, tiled=True),
        preferred_element_type=jnp.float32,
    )
    up_part = jnp.dot(
        columns, lax.all_gather(w_up, "sp", axis=0, tiled=True), preferred_element_type=jnp.float32
    )
    hidden = (jax.nn.silu(gate) * up_part).astype(jnp.bfloat16)
    terms = jnp.dot(
        hidden, lax.all_gather(w_down, "sp", axis=1, tiled=True), preferred_element_type=jnp.float32
    )
    down = lax.psum_scatter(
        terms.astype(jnp.bfloat16), "tp", scatter_dimension=0, tiled=True
    ).astype(jnp.float32)
    return (mid + 0.5 * down).astype(jnp.bfloat16)


MESH = pl.DeviceIdType.MESH
BLOCK = 128


def line_of_chips(mesh):
    count = mesh.shape["sp"]
    try:
        places = [(tuple(d.coords), d.core_on_chip) for d in mesh.devices[:, 0].flat]
    except AttributeError:
        return None
    if count % 4 or count < 12 or mesh.shape["tp"] != 2:
        return None
    first = places[0][0]
    for at, (coords, core) in enumerate(places):
        chip = at // 2
        want = (first[0], first[1] + chip % 2, first[2] + chip // 2)
        if coords != want or core != at % 2:
            return None
    return count // 4


def message_count(n):
    events = 2 * (n - 1)
    keys_and_values = 2 * events + 2 * (events + 1) + 1
    weights = 3 * n + 9 * n + 4
    return keys_and_values + weights + 1 + 2 * events + 8 * (n - 1)


def turned_heads(head_size, x_ref, g_ref, cos_ref, sin_ref):
    x = x_ref[...].astype(jnp.float32)
    width = x.shape[1]
    lane = lax.broadcasted_iota(jnp.int32, (width, width), 0) // head_size
    other = lax.broadcasted_iota(jnp.int32, (width, width), 1) // head_size
    same = (lane == other).astype(jnp.float32)
    mean = jnp.dot(
        x * x, same, preferred_element_type=jnp.float32, precision=lax.Precision.HIGHEST
    ) * (1.0 / head_size)
    h = x * lax.rsqrt(mean + EPS) * jnp.concatenate([g_ref[...]] * (width // head_size), axis=1)
    quarter = head_size // 4
    repeats = width // cos_ref.shape[1]
    cos_table = jnp.concatenate([cos_ref[...]] * repeats, axis=1)
    sin_table = jnp.concatenate([sin_ref[...]] * repeats, axis=1)
    at = lax.broadcasted_iota(jnp.int32, x.shape, 1)
    is_first = (at // quarter) % 2 == 0
    ahead = pltpu.roll(h, width - quarter, 1)
    behind = pltpu.roll(h, quarter, 1)
    turned = h * cos_table + jnp.where(is_first, -ahead, behind) * sin_table
    return turned.astype(jnp.bfloat16)


def when(condition, action):
    if condition is None:
        action()
    else:
        pl.when(condition)(action)


def both(one, other):
    if one is None:
        return other
    if other is None:
        return one
    return jnp.logical_and(one, other)


def layer_kernel(
    n, head_size,
    raw_q, raw_k, raw_v, qg_ref, kg_ref, freq_ref, res_ref, gain_ref, wo_in, wg_in, wu_in, wd_in,
    out_ref,
    q_ref, kv_all, wg_all, wu_all, wd_all, wo_own, attn, context, proj_out, proj_in, mid, normed, hidden,
    part, leaving, line_in, out_own, cos_ref, sin_ref, own_sem, out_sem, send_sem, recv_sem,
):
    sp = lax.axis_index("sp")
    tp = lax.axis_index("tp")
    core = lax.rem(sp, 2)
    y = lax.rem(lax.div(sp, 2), 2)
    z = lax.div(sp, 4)

    def device(zz, yy, cc):
        return (zz * 2 + yy) * 2 + cc

    def wrapped(zz):
        return lax.rem(zz + n, n)

    sibling = (device(z, y, 1 - core), tp)
    across = (device(z, 1 - y, core), tp)
    partner = (sp, 1 - tp)

    def level(zz):
        return (device(zz, y, core), tp)

    barrier = pltpu.get_barrier_semaphore()
    greeted = [sibling, across, partner] + [level(wrapped(z + d)) for d in range(1, n)]
    for target in greeted:
        pl.semaphore_signal(barrier, inc=1, device_id=target, device_id_type=MESH)
    pl.semaphore_wait(barrier, len(greeted))

    slots = {}
    sent = []

    def message(key, src, dst, target):
        slot = key
        if isinstance(key, tuple):
            slot = slots.setdefault(key, 3 * n + len(slots))
        return pltpu.make_async_remote_copy(
            src_ref=src, dst_ref=dst, send_sem=send_sem.at[0], recv_sem=recv_sem.at[slot],
            device_id=target, device_id_type=MESH,
        )

    def send(key, condition, src, dst, target):
        def make():
            return message(key, src(), dst(), target)

        when(condition, lambda: make().start())
        sent.append((condition, make))

    def land(key, condition, piece):
        when(condition, lambda: message(key, piece(), piece(), partner).wait_recv())

    near = [z]
    for p in range(1, n):
        level_at = 0
        for zz in range(n):
            order = sorted(range(n), key=lambda other: (abs(other - zz), -abs(2 * other - n + 1)))
            level_at = jnp.where(z == zz, order[p], level_at)
        near.append(level_at)

    arrivals = [[(s, w) for w in range(2)] for s in range(n - 1)]
    events = [None] + [e for step in arrivals for e in step]
    room = (z <= n - 2, z >= 1)
    ahead = (level(z + 1), level(z - 1))

    def home(e):
        if e is None:
            return z
        return z - 1 - e[0] if e[1] == 0 else z + 1 + e[0]

    def real(e):
        if e is None:
            return None
        return z >= e[0] + 1 if e[1] == 0 else z <= n - 2 - e[0]

    def pass_on(name, e, src, dst):
        for w in range(2) if e is None else (e[1],):
            step = 0 if e is None else e[0] + 1
            if step <= n - 2:
                send((name, step, w), both(real(e), room[w]), src, dst, ahead[w])

    tok = raw_q.shape[0]
    kv_width = raw_k.shape[1]

    def kv_piece(j, zz, yy, cc):
        start = pl.multiple_of(device(zz, yy, cc) * tok, tok)
        return kv_all.at[pl.ds(start, tok), j * kv_width:(j + 1) * kv_width]

    def kv_serve(j, e):
        def dst():
            return kv_piece(j, home(e), y, core)

        if e is not None:
            land((("kv", j), e[0], e[1]), real(e), dst)
        src = (lambda: raw_v) if e is None and j == 1 else dst
        pass_on(("kv", j), e, src, dst)
        send(("kv y", j, e), real(e), src, dst, across)
        send(("kv core",), real(e), src, dst, sibling)

    def kv_cross(j, e):
        def piece():
            return kv_piece(j, home(e), 1 - y, core)

        land(("kv y", j, e), real(e), piece)
        send(("kv core",), real(e), piece, piece, sibling)

    def kv_finish():
        land(("kv core",), None, lambda: kv_all.at[:kv_all.shape[0] // 2, :])

    GATE, UP, DOWN = range(3)
    weights_in = (wg_in, wu_in, wd_in)
    rows, units = wg_in.shape
    lanes_down = wd_in.shape[1]
    slab = wg_all.shape[1]
    share = slab // BLOCK

    def first_block(zz, xx):
        return lax.div(zz * share + xx, 2)

    def unit_forms(zz, xx):
        if share % 2 == 0:
            return [(None, share // 2)]
        many = lax.rem(zz + xx, 2) == 1
        return [(jnp.logical_not(many), share // 2), (many, share // 2 + 1)]

    def weight_in(k, zz, count):
        span = pl.ds(pl.multiple_of(first_block(zz, tp) * BLOCK, BLOCK), count * BLOCK)
        return wd_in.at[span, :] if k == DOWN else weights_in[k].at[:, span]

    def weight(k, xx, zz, yy, cc, keeper, count):
        o = device(zz, yy, cc)
        before = xx * (first_block(keeper + 1, 0) - first_block(keeper, 0))
        units_of = pl.ds(pl.multiple_of(before * BLOCK, BLOCK), count * BLOCK)
        if k == DOWN:
            return wd_all.at[units_of, pl.ds(pl.multiple_of(o * lanes_down, lanes_down), lanes_down)]
        return (wg_all, wu_all)[k].at[pl.ds(pl.multiple_of(o * rows, rows), rows), units_of]

    def weight_line(k, p):
        zt = near[p]
        for condition, count in unit_forms(zt, tp):
            send(
                k * n + wrapped(zt - z), condition,
                functools.partial(weight_in, k, zt, count),
                functools.partial(weight, k, tp, z, y, core, zt, count), level(zt),
            )

    def by_x(k, p):
        return (p % 4 < 2, p % 2 == 0, p % 4 < 2)[k]

    def weight_move(k, p, xx, yy, way):
        target = {"x": partner, "y": across, "core": sibling}[way]
        corner = (xx is not tp, yy is not y)
        for condition, count in unit_forms(z, xx):
            dst = functools.partial(weight, k, xx, near[p], yy, core, z, count)
            src = dst
            if p == 0 and corner == (False, False):
                src = functools.partial(weight_in, k, z, count)
            key = ("w", way, k, p, corner)
            if way == "core":
                key = ("w", way, k, k == DOWN and corner[1])
            send(key, condition, src, dst, target)

    other_x, other_y = 1 - tp, 1 - y

    def weight_take(key, k, p, xx, yy, cc):
        for condition, count in unit_forms(z, xx):
            land(key, condition, functools.partial(weight, k, xx, near[p], yy, cc, z, count))

    def weight_land(k, p, way, xx, yy):
        corner = (xx is not tp, yy is not y)
        seen = {"x": (not corner[0], corner[1]), "y": (corner[0], not corner[1])}[way]
        weight_take(("w", way, k, p, seen), k, p, xx, yy, core)

    def weight_arrive(k, p):
        weight_take(k * n + wrapped(z - near[p]), k, p, tp, y, core)

    def weight_serve(k, p):
        if p > 0:
            weight_arrive(k, p)
        weight_move(k, p, tp, y, "y")
        weight_move(k, p, tp, y, "x")
        weight_move(k, p, tp, y, "core")

    def cross_y(k, p):
        weight_land(k, p, "y", tp, other_y)
        if by_x(k, p):
            weight_move(k, p, tp, other_y, "x")
        weight_move(k, p, tp, other_y, "core")

    def cross_x(k, p):
        weight_land(k, p, "x", other_x, y)
        if not by_x(k, p):
            weight_move(k, p, other_x, y, "y")
        weight_move(k, p, other_x, y, "core")

    def cross_both(k, p):
        weight_land(k, p, "x" if by_x(k, p) else "y", other_x, other_y)
        weight_move(k, p, other_x, other_y, "core")

    def own_copy(k, count):
        return pltpu.make_async_copy(
            weight_in(k, z, count), weight(k, tp, z, y, core, z, count), own_sem.at[k]
        )

    def own_each(act):
        for k in range(3):
            for condition, count in unit_forms(z, tp):
                when(condition, lambda: act(own_copy(k, count)))

    own_wo = pltpu.make_async_copy(wo_in, wo_own, own_sem.at[3])

    def weight_finish(k, second=False):
        def bulk():
            if k == DOWN:
                return wd_all.at[:, :wd_all.shape[1] // 4]
            ref = (wg_all, wu_all)[k]
            return ref.at[:ref.shape[0] // 2, :]

        land(("w", "core", k, second), None, bulk)

    pairs, q_rows, lanes = q_ref.shape
    block = math.gcd(q_rows, 256)
    per_pair = q_rows // block

    def attend(at):
        pair, which = at // per_pair, at % per_pair
        span = slice(which * block, (which + 1) * block)
        q = q_ref[pair, span, :]
        k = kv_all[:, pair * lanes:(pair + 1) * lanes]
        v = kv_all[:, (pairs + pair) * lanes:(pairs + pair + 1) * lanes]
        scores = lax.dot_general(
            q, k, (((1,), (1,)), ((), ())), preferred_element_type=jnp.float32
        )
        weights = jnp.exp(scores - jnp.max(scores, axis=-1, keepdims=True))
        total = jnp.sum(weights, axis=-1, keepdims=True)
        mixed = jnp.dot(weights.astype(jnp.bfloat16), v, preferred_element_type=jnp.float32)
        attn[pair, span, :] = (mixed / total).astype(jnp.bfloat16)

    def assemble():
        group = q_rows // (2 * tok)
        pieces = []
        for pair in range(pairs):
            for side in range(2):
                for g in range(0, group, 2):
                    lower = attn[pair, pl.ds((side * group + g) * tok, tok), :].astype(jnp.float32)
                    upper = attn[pair, pl.ds((side * group + g + 1) * tok, tok), :].astype(jnp.float32)
                    if side == 1:
                        lower = pltpu.roll(lower, head_size, 1)
                    else:
                        upper = pltpu.roll(upper, head_size, 1)
                    lane = lax.broadcasted_iota(jnp.int32, lower.shape, 1)
                    pieces.append(jnp.where(lane < head_size, lower, upper).astype(jnp.bfloat16))
        context[...] = jnp.concatenate(pieces, axis=1)

    own_count, width = res_ref.shape
    rows_of = own_count // 2
    mine = pl.ds(pl.multiple_of(tp * own_count, own_count), own_count)
    theirs = pl.ds(pl.multiple_of((1 - tp) * own_count, own_count), own_count)

    def whole(zz):
        return pl.ds(pl.multiple_of(zz * own_count, own_count), own_count)

    def rows_at(zz, f):
        return pl.ds(pl.multiple_of((zz * 2 + f) * rows_of, rows_of), rows_of)

    wide = math.gcd(width, 512)

    def project():
        given = context[theirs, :]
        for at in range(0, width, wide):
            cols = slice(at, at + wide)
            proj_out[:, cols] = jnp.dot(
                given, wo_own[:, cols], preferred_element_type=jnp.float32
            ).astype(jnp.bfloat16)

    def project_own():
        held = context[mine, :]
        for at in range(0, width, wide):
            cols = slice(at, at + wide)
            mid[:, cols] = res_ref[:, cols].astype(jnp.float32) + jnp.dot(
                held, wo_own[:, cols], preferred_element_type=jnp.float32
            )

    def normalize():
        value = mid[...] + proj_in[...].astype(jnp.float32)
        mid[...] = value
        scale = lax.rsqrt(jnp.mean(value * value, axis=-1, keepdims=True) + EPS)
        normed[whole(z), :] = (value * scale * gain_ref[...]).astype(jnp.bfloat16)

    def rows_serve(f, e):
        def piece():
            return normed.at[rows_at(home(e), f), :]

        if e is not None:
            land((("rows", f), e[0], e[1]), real(e), piece)
        pass_on(("rows", f), e, piece, piece)

    tile = 2 * lanes_down

    def feed():
        def some(cols):
            x = normed[...]
            gate = jnp.dot(x, wg_all[:, cols], preferred_element_type=jnp.float32)
            up = jnp.dot(x, wu_all[:, cols], preferred_element_type=jnp.float32)
            hidden[:, cols] = (gate / (1.0 + jnp.exp(-gate)) * up).astype(jnp.bfloat16)

        @pl.loop(0, slab // tile)
        def _(at):
            some(pl.ds(pl.multiple_of(at * tile, tile), tile))

        if slab % tile:
            some(slice(slab - slab % tile, slab))

    groups = 4
    cols_of = width // groups

    def result_columns(g, at):
        zs = g % 2 * (n // 2) + at
        start = (zs * 4 + 2 * (y, other_y)[g // 2]) * lanes_down
        return pl.ds(pl.multiple_of(start, tile), tile)

    def lower(g):
        @pl.loop(0, n // 2)
        def _(at):
            cols = pl.ds(pl.multiple_of(g * cols_of + at * tile, tile), tile)
            part[:, cols] = jnp.dot(
                hidden[...], wd_all[:, result_columns(g, at)], preferred_element_type=jnp.float32
            )

    def columns(g):
        return slice(g * cols_of, (g + 1) * cols_of)

    def add(zz, f, ref):
        part[whole(zz), columns(f)] = part[whole(zz), columns(f)] + ref[...].astype(jnp.float32)

    def sum_step(f, d, ends=None):
        for w in range(2):
            inside = z <= n - 1 - d if w == 0 else z >= d
            if ends is not None:
                inside = both(inside, jnp.logical_not(room[1 - w]) if ends else room[1 - w])
            sum_send(f, w, d, inside)

    def sum_send(f, w, d, inside):
        zz = z + d if w == 0 else z - d
        if d < n - 1:
            def take():
                message(("sum", f, w, d + 1), line_in.at[f, w, d], line_in.at[f, w, d], partner).wait_recv()
                add(zz, f, line_in.at[f, w, d])

            when(both(inside, room[1 - w]), take)

        def put():
            leaving[whole(zz), columns(f)] = part[whole(zz), columns(f)].astype(jnp.bfloat16)

        when(inside, put)
        send(
            ("sum", f, w, d), inside,
            lambda: leaving.at[whole(zz), columns(f)], lambda: line_in.at[f, w, d - 1], ahead[w],
        )

    def out_copy(g, at):
        cols = result_columns(g, at)
        return pltpu.make_async_copy(
            out_own.at[:, cols], out_ref.at[:, cols], out_sem.at[g * (n // 2) + at]
        )

    def sum_finish(f):
        for w in range(2):
            def take():
                message(("sum", f, w, 1), line_in.at[f, w, 0], line_in.at[f, w, 0], partner).wait_recv()
                add(z, f, line_in.at[f, w, 0])

            when(room[1 - w], take)
        for at in range(n // 2):
            cols = result_columns(f, at)
            start = f * cols_of + at * tile
            down = part[whole(z), start:start + tile]
            out_own[:, cols] = (mid[:, cols] + 0.5 * down).astype(jnp.bfloat16)
            out_copy(f, at).start()

    own_each(lambda copy: copy.start())
    own_wo.start()
    kv_serve(1, None)
    own_rows = pl.ds(pl.multiple_of(sp * tok, tok), tok)
    at_row = (sp * tok + lax.broadcasted_iota(jnp.int32, cos_ref.shape, 0)).astype(jnp.float32)
    grid_row = jnp.floor(at_row * (1.0 / GRID_W))
    lane = lax.broadcasted_iota(jnp.int32, cos_ref.shape, 1)
    by_row = jnp.bitwise_and(lane, head_size - 1) < head_size // 2
    angle = jnp.where(by_row, grid_row, at_row - GRID_W * grid_row) * freq_ref[...]
    cos_ref[...] = jnp.cos(angle)
    sin_ref[...] = jnp.sin(angle)
    kv_all[own_rows, :kv_width] = turned_heads(head_size, raw_k, kg_ref, cos_ref, sin_ref)
    kv_all[own_rows, kv_width:] = raw_v[...]
    for k in range(3):
        weight_move(k, 0, tp, y, "x")
        weight_move(k, 0, tp, y, "core")
    kv_serve(0, None)
    weight_move(GATE, 0, tp, y, "y")
    for p in range(1, n):
        weight_line(GATE, p)
    turned = turned_heads(head_size, raw_q, qg_ref, cos_ref, sin_ref).astype(jnp.float32)
    turned = turned * head_size ** (-0.5)
    group = q_rows // (2 * tok)
    for at in range(raw_q.shape[1] // lanes):
        together = turned[:, at * lanes:(at + 1) * lanes]
        swapped = pltpu.roll(together, head_size, 1)
        low = lax.broadcasted_iota(jnp.int32, together.shape, 1) < head_size
        key_head, g = 2 * at // group, 2 * at % group
        pair, side = key_head // 2, key_head % 2
        for extra in range(2):
            source = together if extra == side else swapped
            kept_lanes = jnp.where(low if side == 0 else jnp.logical_not(low), source, 0.0)
            first = (side * group + g + extra) * tok
            q_ref[pair, first:first + tok, :] = kept_lanes.astype(jnp.bfloat16)

    def all_lines(k):
        for p in range(2 if k == UP else 1, n):
            weight_line(k, p)

    serve = [(k, d) for k in range(3) for d in range(1, n)]
    over_both = [(k, d) for k in range(3) for d in range(n)]
    over_x = sorted(over_both, key=lambda what: what[1] > 0)
    over_y = list(over_x)
    queues = {"s": (weight_serve, serve), "x": (cross_x, over_x), "y": (cross_y, over_y), "b": (cross_both, over_both), "l": (all_lines, [(UP,), (DOWN,)])}

    def work(plan):
        for letter in plan:
            task, queue = queues[letter]
            if queue:
                task(*queue.pop(0))

    crossing = [None]
    for at, step in enumerate(arrivals):
        for j in (1, 0):
            for e in step:
                kv_serve(j, e)
        if at == 0:
            weight_move(UP, 0, tp, y, "y")
        work(("", "xys", "ssl")[max(0, at - n + 4)])
        if at == n - 3:
            weight_line(UP, 1)
        for j in (1, 0):
            for e in crossing:
                kv_cross(j, e)
        if at == n - 3:
            work("xy")
        crossing = step
    for j in (1, 0):
        for e in crossing:
            kv_cross(j, e)
    weight_move(DOWN, 0, tp, y, "y")
    kv_finish()
    plans = ["", "", "", "s", "", "l"]
    for at in range(pairs * per_pair):
        attend(at)
        work(plans[at % len(plans)])
    assemble()
    own_wo.wait()
    project()
    send(("proj",), None, lambda: proj_out, lambda: proj_in, partner)
    project_own()
    work("xyxyxyxys")
    land(("proj",), None, lambda: proj_in)
    normalize()
    for f in range(2):
        rows_serve(f, None)

    def rows_step(at):
        for f in range(2):
            for e in arrivals[at]:
                rows_serve(f, e)

    work("xysxy")
    rows_step(0)
    work("xyss")
    while over_both[0][0] < UP:
        work("b")
    rows_step(1)
    work("s")
    while over_both[0][0] < DOWN:
        work("b")
    own_each(lambda copy: copy.wait())
    weight_finish(GATE)
    weight_finish(UP)
    for at in range(2, n - 1):
        rows_step(at)
    work("xy")
    feed()
    work("xy" * len(over_x))
    weight_finish(DOWN)
    for g in (0, 1):
        lower(g)
        sum_step(g, n - 1)
    for g in (0, 1):
        sum_step(g, n - 2)
    work("b" * len(over_both))
    weight_finish(DOWN, True)
    for g in (2, 3):
        lower(g)
        sum_step(g, n - 1)
    for two in ((0, 1), (2, 3)):
        for d in range(n - 2, 0, -1):
            for g in two:
                if d < n - 2 or g > 1:
                    sum_step(g, d, False if d == 1 else None)
    for g in range(groups):
        sum_step(g, 1, True)
    for g in range(groups):
        sum_finish(g)
    for g in range(groups):
        for at in range(n // 2):
            out_copy(g, at).wait()
    for condition, make in sent:
        when(condition, lambda: make().wait_send())
    assert len(slots) + 3 * n == recv_sem.shape[0]


def fast_body(n, queries, keys, values, q_gain, k_gain, w_out, residual, norm_gain, w_gate, w_up, w_down):
    tok_rows = queries.shape[0]
    head_size = q_gain.shape[0]
    q_heads = queries.shape[1] // head_size
    kv_heads = keys.shape[1] // head_size
    q_group = q_heads // kv_heads
    if 2 * w_gate.shape[1] % (n * BLOCK) or n % 2:
        return body(
            queries, keys, values, q_gain, k_gain, w_out, residual, norm_gain, w_gate, w_up, w_down
        )
    n_sp = 4 * n
    half_size = head_size // 2
    inv_freq = np.float32(THETA) ** (-np.arange(0, half_size, 2, dtype=np.float32) / half_size)
    frequencies = jnp.asarray(np.tile(inv_freq, 8)[None, :], jnp.float32)
    pairs = kv_heads // 2
    padded = (pairs, 2 * q_group * tok_rows, 2 * head_size)
    kv_width = keys.shape[1] + values.shape[1]
    tokens = n_sp * tok_rows
    any_space = pl.BlockSpec(memory_space=pl.ANY)
    vmem = pl.BlockSpec(memory_space=pltpu.VMEM)
    own_count, width = residual.shape
    depth_in, units = w_gate.shape
    lanes_down = w_down.shape[1]
    slab = 2 * units // n
    group_rows = n * own_count
    bf16, f32 = jnp.bfloat16, jnp.float32
    return pl.pallas_call(
        functools.partial(layer_kernel, n, head_size),
        out_shape=jax.ShapeDtypeStruct(residual.shape, bf16),
        in_specs=[vmem] * 8 + [any_space] * 4,
        out_specs=any_space,
        scratch_shapes=[
            pltpu.VMEM(padded, bf16),
            pltpu.VMEM((tokens, kv_width), bf16),
            pltpu.VMEM((n_sp * depth_in, slab), bf16),
            pltpu.VMEM((n_sp * depth_in, slab), bf16),
            pltpu.VMEM((slab, n_sp * lanes_down), bf16),
            pltpu.VMEM(w_out.shape, bf16),
            pltpu.VMEM(padded, bf16),
            pltpu.VMEM(queries.shape, bf16),
            pltpu.VMEM((own_count, width), bf16),
            pltpu.VMEM((own_count, width), bf16),
            pltpu.VMEM((own_count, width), f32),
            pltpu.VMEM((group_rows, width), bf16),
            pltpu.VMEM((group_rows, slab), bf16),
            pltpu.VMEM((group_rows, width), f32),
            pltpu.VMEM((group_rows, width), bf16),
            pltpu.VMEM((4, 2, n - 1, own_count, width // 4), bf16),
            pltpu.VMEM((own_count, width), bf16),
            pltpu.VMEM((tok_rows, 2 * head_size), f32),
            pltpu.VMEM((tok_rows, 2 * head_size), f32),
            pltpu.SemaphoreType.DMA((4,)),
            pltpu.SemaphoreType.DMA((2 * n,)),
            pltpu.SemaphoreType.DMA((1,)),
            pltpu.SemaphoreType.DMA((message_count(n),)),
        ],
        compiler_params=pltpu.CompilerParams(
            collective_id=0, has_side_effects=True, vmem_limit_bytes=63 * 1024 * 1024
        ),
        name="layer",
    )(
        queries, keys, values, q_gain[None, :], k_gain[None, :], frequencies,
        residual, norm_gain[None, :], w_out, w_gate, w_up, w_down)


def solution(mesh):
    n = line_of_chips(mesh)
    inner = body if n is None else functools.partial(fast_body, n)
    return jax.shard_map(
        inner,
        mesh=mesh,
        in_specs=(
            P("sp", "tp"),
            P("sp", "tp"),
            P("sp", "tp"),
            P(),
            P(),
            P("tp", None),
            P(("sp", "tp"), None),
            P(),
            P("sp", "tp"),
            P("sp", "tp"),
            P("tp", "sp"),
        ),
        out_specs=P(("sp", "tp"), None),
        check_vma=False,
    )
```
